512 devices in a mesh: sp: 16 (over z), fs: 4 (over y), tp: 8 (over x, core).
Axes of the slice: x: 4, y: 4, z: 16, core: 2. Of those that a mesh axis runs over, the one named last changes fastest.
Arguments:
- tokens: bfloat16 [16384, 2048], P(('fs', 'sp', 'tp')), parts along dimension 0, may hold values from -6 to 6
- norm_gain: float32 [2048], replicated, may hold values from 0.1 to 1.9
- recurrent_input: bfloat16 [2048, 1024], P(None, 'tp'), may hold values from -0.125 to 0.125
- recurrent_gate: bfloat16 [2048, 1024], P(None, 'tp'), may hold values from -0.125 to 0.125
- attention_gate: bfloat16 [2048, 1024], P(None, 'tp'), may hold values from -0.125 to 0.125
- query_proj: bfloat16 [2048, 1536], P(None, 'tp'), may hold values from -0.125 to 0.125
- latent_down: bfloat16 [2048, 512], P(None, 'tp'), may hold values from -0.125 to 0.125
- rope_key_down: bfloat16 [2048, 64], replicated, may hold values from -0.125 to 0.125
- conv_kernel: float32 [4, 1024], P(None, 'tp'), may hold values from -3 to 3
- recurrence_gate_blocks: bfloat16 [16, 64, 64], P('tp'), may hold values from -0.75 to 0.75
- input_gate_blocks: bfloat16 [16, 64, 64], P('tp'), may hold values from -0.75 to 0.75
- decay_rate: float32 [1024], P('tp'), as said below
- decay_shift: float32 [16384], P(('fs', 'sp')), parts along dimension 0, may hold values from -2 to 0, as said below
- initial_state: float32 [4096], P(('fs', 'tp')), parts along dimension 0, may hold values from -6 to 6
- latent_gain: float32 [512], replicated, may hold values from 0.1 to 1.9
- latent_up: bfloat16 [512, 2048], P(None, 'tp'), may hold values from -0.25 to 0.25
- query_gain: float32 [192], replicated, may hold values from 0.4 to 250, as said below
- recurrent_output: bfloat16 [1024, 2048], P('tp'), may hold values from -0.25 to 0.25
- attention_output: bfloat16 [1024, 2048], P('tp'), may hold values from -0.25 to 0.25
Outputs:
- mixed_output: bfloat16 [16384, 2048], P(('fs', 'sp', 'tp')), parts along dimension 0
The draws below stay inside these ranges and needn't reach their ends.
There are 4 independent parts, one for each index of `fs`. The reference program is written for one: setup_inputs(seed, part) draws one part's arguments, and reference() takes and returns one part's arrays. A program takes and returns all parts, laid end to end along the dimension named above; an argument that names none is the same for every part. Nothing has to cross between parts.
Inputs may be any that keep to these rules, and one draw needn't show every extreme that they name: `decay_rate`: positive. `decay_shift`: negative. `query_gain`: positive.
All inputs are finite; a program needn't handle non-finite values.
Results may differ from the reference program's by a relative error of at most 0.03.
The reference program's roundings to bfloat16 on the way count: a program that leaves them out, or rounds other values in their place, can miss the bound.
Values may be sent and summed in bfloat16 or wider, within the bound.
A program may use at most 64 MiB of HBM per device.

```python
import math
import jax
import jax.numpy as jnp
from jax import lax

D = 2048
DR = 1024
BLK = 64
BLOCKS = 16
CONV = 4
H = 8
NOPE = 128
ROPE = 64
VH = 128
LAT = 512
DA = 1024
TOK_DEV = 256
SEQUENCE_LENGTH = 4096
N_TP = 8


def draw_decay_rate(key, part):
    pick_key, slow_key, fast_key = jax.random.split(key, 3)
    slow_share = 0.5
    slow_mask = jax.random.bernoulli(pick_key, slow_share, (DR,))
    slow_rate = jnp.exp(jax.random.uniform(slow_key, (DR,), jnp.float32, jnp.log(0.05), jnp.log(1.0))) / (8.0 * SEQUENCE_LENGTH)
    fast_rate = jnp.exp(jax.random.uniform(fast_key, (DR,), jnp.float32, jnp.log(0.004), jnp.log(0.012)))
    return jnp.where(slow_mask, slow_rate, fast_rate)


def draw_decay_shift(key, part):
    level_key, place_key, depth_key = jax.random.split(key, 3)
    block_count = SEQUENCE_LENGTH // TOK_DEV
    levels = jnp.exp(jax.random.uniform(level_key, (block_count,), jnp.float32, jnp.log(0.05), jnp.log(0.5))) / SEQUENCE_LENGTH
    baseline_offset = -jnp.repeat(levels, TOK_DEV)
    slot_indices = jax.random.randint(place_key, (2,), 0, SEQUENCE_LENGTH)
    layer_depths = jnp.log(jax.random.uniform(depth_key, (2,), jnp.float32, 0.5, 0.8))
    spike_flags = jnp.arange(SEQUENCE_LENGTH)[:, None] == slot_indices[None, :]
    return baseline_offset + jnp.sum(jnp.where(spike_flags, layer_depths[None, :], 0.0), axis=1)


def draw_query_gain(key, part):
    gain_key = jax.random.fold_in(key, 0)
    gain_values = jax.random.uniform(gain_key, (NOPE + ROPE,), jnp.float32, 0.4, 1.6)
    return gain_values


def level_of(rng, extent, cuts, least, high):
    level = 1.0
    for axis_at, parts in cuts:
        heights = jax.random.uniform(jax.random.fold_in(jax.random.fold_in(rng, 6), axis_at), (parts,), jnp.float32, least / len(cuts), high / len(cuts))
        level = level * jnp.repeat(jnp.exp(heights), extent[axis_at] // parts).reshape((-1,) + (1,) * (len(extent) - 1 - axis_at))
    return level


def scatter_about(key, extent, scale, bound, cuts=(), kind=jnp.bfloat16):
    array = scale * jax.random.normal(key, extent, jnp.float32)
    if cuts:
        array = array * level_of(key, extent, cuts, -0.22, 0.18)
    return jnp.clip(array, -bound, bound).astype(kind)


def setup_inputs(seed: int = 0, part: int = 0) -> dict:
    splits = jax.random.split(jax.random.key(seed), 20)
    part_keys = jax.random.split(jax.random.fold_in(splits[19], part), 20)
    return {
        "tokens": scatter_about(part_keys[0], (SEQUENCE_LENGTH, D), 1.0, 6.0, ((0, 128),)),
        "norm_gain": jnp.clip(1.0 + 0.18 * jax.random.normal(splits[1], (D,), jnp.float32), 0.1, 1.9),
        "recurrent_input": scatter_about(splits[2], (D, DR), D ** -0.5, 0.125, ((1, 8),)),
        "recurrent_gate": scatter_about(splits[3], (D, DR), D ** -0.5, 0.125, ((1, 8),)),
        "attention_gate": scatter_about(splits[4], (D, DA), D ** -0.5, 0.125, ((1, 8),)),
        "query_proj": scatter_about(splits[5], (D, H * (NOPE + ROPE)), D ** -0.5, 0.125, ((1, 8),)),
        "latent_down": scatter_about(splits[6], (D, LAT), D ** -0.5, 0.125, ((1, 8),)),
        "rope_key_down": scatter_about(splits[7], (D, ROPE), D ** -0.5, 0.125),
        "conv_kernel": scatter_about(splits[8], (CONV, DR), 0.5, 3.0, ((1, 8),), jnp.float32),
        "recurrence_gate_blocks": scatter_about(splits[9], (BLOCKS, BLK, BLK), BLK ** -0.5, 0.75, ((0, 8),)),
        "input_gate_blocks": scatter_about(splits[10], (BLOCKS, BLK, BLK), BLK ** -0.5, 0.75, ((0, 8),)),
        "decay_rate": draw_decay_rate(jax.random.fold_in(splits[19], 71), part),
        "decay_shift": draw_decay_shift(jax.random.fold_in(jax.random.fold_in(splits[19], part), 71), part),
        "initial_state": scatter_about(part_keys[13], (DR,), 1.0, 6.0, ((0, 8),), jnp.float32),
        "latent_gain": jnp.clip(1.0 + 0.18 * jax.random.normal(splits[14], (LAT,), jnp.float32), 0.1, 1.9),
        "latent_up": scatter_about(splits[15], (LAT, H * (NOPE + VH)), LAT ** -0.5, 0.25, ((1, 8),)),
        "query_gain": draw_query_gain(jax.random.fold_in(splits[19], 71), part),
        "recurrent_output": scatter_about(splits[17], (DR, D), ((DR + DA) // 4) ** -0.5, 0.25, ((0, 8),)),
        "attention_output": scatter_about(splits[18], (DA, D), ((DR + DA) // 4) ** -0.5, 0.25, ((0, 8),)),
    }


EPS = 1e-06
RECURRENT_SCALE = 8.0
THETA = 10000.0

def rotate_half(values, token_positions):
    half_width = values.shape[-1] // 2
    inv_freq = 1.0 / THETA ** (jnp.arange(0, 2 * half_width, 2, dtype=jnp.float32) / (2 * half_width))
    angles = token_positions.astype(jnp.float32)[:, None] * inv_freq[None, :]
    cosine = jnp.cos(angles)
    sine_part = jnp.sin(angles)
    if values.ndim == 3:
        cosine = cosine[:, None, :]
        sine_part = sine_part[:, None, :]
    first_half = values[..., :half_width]
    second_half = values[..., half_width:]
    return jnp.concatenate([first_half * cosine - second_half * sine_part, first_half * sine_part + second_half * cosine], axis=-1)

def rms_scaled(values, gain_vec):
    return values * lax.rsqrt(lax.optimization_barrier(jnp.mean(values * values, axis=-1, keepdims=True)) + EPS) * gain_vec

def rounded(values):
    return lax.optimization_barrier(values.astype(jnp.bfloat16)).astype(jnp.float32)

def linear_step(earlier, later_part):
    return (earlier[0] * later_part[0], later_part[0] * earlier[1] + later_part[1])

def reference(tokens, norm_gain, recurrent_input, recurrent_gate, attention_gate, query_proj, latent_down, rope_key_down, conv_kernel, recurrence_gate_blocks, input_gate_blocks, decay_rate, decay_shift, initial_state, latent_gain, latent_up, query_gain, recurrent_output, attention_output):
    normed = rms_scaled(tokens.astype(jnp.float32), norm_gain).astype(jnp.bfloat16)

    def project(weight):
        return jnp.dot(normed, weight, preferred_element_type=jnp.float32).astype(jnp.bfloat16)
    recur_signal = project(recurrent_input)
    recur_gate_pre = project(recurrent_gate)
    attention_pre = project(attention_gate)
    query_raw = project(query_proj)
    latent_raw = project(latent_down)
    rope_raw = project(rope_key_down)
    token_positions = jnp.arange(SEQUENCE_LENGTH, dtype=jnp.int32)
    padded = jnp.concatenate([jnp.zeros((CONV - 1, DR), jnp.bfloat16), recur_signal], axis=0).astype(jnp.float32)
    conv_sum = conv_kernel[0] * padded[0:SEQUENCE_LENGTH]
    for tap_index in range(1, CONV):
        conv_sum = conv_sum + conv_kernel[tap_index] * padded[tap_index:tap_index + SEQUENCE_LENGTH]
    conv_back = rounded(conv_sum)
    grouped = conv_back.reshape(SEQUENCE_LENGTH, BLOCKS, BLK)
    recur_rate = jax.nn.sigmoid(jnp.einsum('tbi,bij->tbj', grouped, recurrence_gate_blocks.astype(jnp.float32)).reshape(SEQUENCE_LENGTH, DR))
    input_rate = jax.nn.sigmoid(jnp.einsum('tbi,bij->tbj', grouped, input_gate_blocks.astype(jnp.float32)).reshape(SEQUENCE_LENGTH, DR))
    log_decay = -RECURRENT_SCALE * recur_rate * decay_rate + decay_shift[:, None]
    decay = jnp.exp(log_decay)
    driven = jnp.sqrt(-jnp.expm1(2.0 * log_decay)) * input_rate * conv_back
    driven = driven.at[0].add(decay[0] * initial_state)
    decay_prod, states = lax.associative_scan(linear_step, (decay, driven), axis=0)
    recur_out = (states * jax.nn.silu(recur_gate_pre.astype(jnp.float32))).astype(jnp.bfloat16)
    query_rows = rms_scaled(query_raw.astype(jnp.float32).reshape(SEQUENCE_LENGTH, H, NOPE + ROPE), query_gain)
    query_rows = jnp.concatenate([query_rows[..., :NOPE], rotate_half(query_rows[..., NOPE:], token_positions)], axis=-1).astype(jnp.bfloat16)
    latent = rms_scaled(latent_raw.astype(jnp.float32), latent_gain).astype(jnp.bfloat16)
    key_values = jnp.dot(latent, latent_up, preferred_element_type=jnp.float32).astype(jnp.bfloat16).reshape(SEQUENCE_LENGTH, H, NOPE + VH)
    key_nope = key_values[..., :NOPE].astype(jnp.float32)
    values_all = key_values[..., NOPE:].astype(jnp.float32)
    key_rope = rotate_half(rope_raw.astype(jnp.float32), token_positions).astype(jnp.bfloat16).astype(jnp.float32)
    query_block = math.gcd(SEQUENCE_LENGTH, 512)
    score_scale = (NOPE + ROPE) ** (-0.5)

    def attend(block_index):
        begin_row = (block_index * query_block).astype(jnp.int32)
        query_part = lax.dynamic_slice_in_dim(query_rows, begin_row, query_block, 0).astype(jnp.float32)
        scores = jnp.einsum('thd,khd->htk', query_part[..., :NOPE], key_nope)
        scores = scores + jnp.einsum('thr,kr->htk', query_part[..., NOPE:], key_rope)
        scores = scores * score_scale
        query_pos = begin_row + jnp.arange(query_block, dtype=jnp.int32)
        allowed = token_positions[None, None, :] <= query_pos[None, :, None]
        scores = jnp.where(allowed, scores, -jnp.inf)
        row_max = lax.optimization_barrier(jnp.max(scores, axis=-1, keepdims=True))
        weights = jnp.exp(scores - row_max)
        denominator = lax.optimization_barrier(jnp.sum(weights, axis=-1))
        weighted = jnp.einsum('htk,khd->thd', rounded(weights), values_all)
        return weighted / jnp.transpose(denominator)[:, :, None]
    attended = lax.map(attend, jnp.arange(SEQUENCE_LENGTH // query_block, dtype=jnp.int32)).reshape(SEQUENCE_LENGTH, DA)
    attention_out = (attended * jax.nn.silu(attention_pre.astype(jnp.float32))).astype(jnp.bfloat16)
    recur_group = DR // N_TP
    attend_group = DA // N_TP

    def add_group(group_index, running):
        index_value = group_index.astype(jnp.int32)
        recur_part = lax.dynamic_slice_in_dim(recur_out, index_value * recur_group, recur_group, 1)
        recur_rows = lax.dynamic_slice_in_dim(recurrent_output, index_value * recur_group, recur_group, 0)
        attend_part = lax.dynamic_slice_in_dim(attention_out, index_value * attend_group, attend_group, 1)
        attend_rows = lax.dynamic_slice_in_dim(attention_output, index_value * attend_group, attend_group, 0)
        partial_sum = jnp.dot(recur_part, recur_rows, preferred_element_type=jnp.float32) + jnp.dot(attend_part, attend_rows, preferred_element_type=jnp.float32)
        return running + rounded(partial_sum)
    total = lax.fori_loop(0, N_TP, add_group, jnp.zeros((SEQUENCE_LENGTH, D), jnp.float32))
    return total.astype(jnp.bfloat16)
```

```python
import functools

import jax
import jax.numpy as jnp
import numpy as np
from jax import lax
from jax.experimental import pallas as pl
from jax.experimental.pallas import tpu as pltpu
from jax.sharding import PartitionSpec as P

MESH = pl.DeviceIdType.MESH
EPS = 1e-06
THETA = 10000.0
F32, BF16 = jnp.float32, jnp.bfloat16
NZ, NX, TOK, D = 16, 4, 256, 2048
PIECES, ROWS = 4, 160
NT = (((1,), (1,)), ((), ()))


def dot(a, b):
    return jnp.dot(a, b, preferred_element_type=F32)


def silu(v):
    return v * jax.nn.sigmoid(v)


def minus_expm1(y):
    series = 1.0 + y * (1.0 / 8.0)
    for n in (7, 6, 5, 4, 3, 2):
        series = 1.0 + y * (1.0 / n) * series
    return jnp.where(y > -0.35, -y * series, 1.0 - jnp.exp(y))


def rotary_tables():
    inv = 1.0 / THETA ** (np.arange(0, 64, 2, dtype=np.float64) / 64)
    lanes = np.tile(inv, 4)

    def table(positions):
        angles = positions[:, None].astype(np.float64) * lanes[None]
        return np.concatenate([np.cos(angles), np.sin(angles)], 1).astype(np.float32)

    return table(np.arange(TOK)), table(TOK * np.arange(NZ))


def kernel(
    tok_h, ngain_h, rin_h, rgate_h, agate_h, wq_h, wlat_h, wrk_h, conv_h, rblk_h, iblk_h,
    drate_h, dshift_h, init_h, lgain_h, lup_h, qgain_h, rout_h, aout_h, base_h, far_h,
    out_ref,
    tok, ngain, wa, wb, wq, wlat, wrk, conv, rblk, iblk, drate, dshift, init, lgain, lup,
    qgain, wo, base, far,
    xbuf, latbuf, halo_tx, halo_rx, kvbuf, cbuf, qn_s, qlo_s, qhi_s, acc_s, ml_s,
    a_s, b_s, gate_s, agate_s, xrow, xcat, d2d_tx, d2d_rx, psum, rtx, rrx,
    in_sem, g_ssem, g_rsem, d_ssem, d_rsem, l_ssem, l_rsem, ld_ssem, ld_rsem, h_sem,
    kv_ssem, kv_rsem, c_ssem, c_rsem, o_ssem, o_rsem, r_ssem, r_rsem,
):
    z = lax.axis_index("sp")
    t = lax.axis_index("tp")
    x, c = lax.div(t, 2), lax.rem(t, 2)

    def chip(offset):
        return lax.rem(x + (offset + NX), NX)

    def tp_of(xx, cc):
        return 2 * xx + cc

    def zat(offset):
        return lax.rem(z + (offset + 2 * NZ), NZ)

    partner = {"tp": tp_of(x, 1 - c)}
    xup, xdn, xfar = ({"tp": tp_of(chip(o), c)} for o in (1, -1, 2))
    zup, zdn = {"sp": zat(1)}, {"sp": zat(-1)}
    started = []

    def remote(src, dst, ssem, rsem, to):
        return pltpu.make_async_remote_copy(
            src_ref=src, dst_ref=dst, send_sem=ssem, recv_sem=rsem, device_id=to,
            device_id_type=MESH,
        )

    def send(src, dst, ssem, rsem, to):
        copy = remote(src, dst, ssem, rsem, to)
        copy.start()
        started.append(copy)

    def arrived(dst, rsem, to=None):
        remote(dst, dst, rsem, rsem, partner).wait_recv()

    barrier = pltpu.get_barrier_semaphore()
    for peer in (partner, xup, xdn, xfar, zup, zdn):
        pl.semaphore_signal(barrier, inc=1, device_id=peer, device_id_type=MESH)

    loads = [
        (tok_h, tok), (ngain_h, ngain), (wq_h, wq), (wlat_h, wlat), (wrk_h, wrk),
        (rin_h, wa.at[:, 0:128]), (rgate_h, wa.at[:, 128:256]), (agate_h, wa.at[:, 256:384]),
        (conv_h, conv), (rblk_h, rblk), (iblk_h, iblk), (drate_h, drate), (dshift_h, dshift),
        (init_h, init), (lgain_h, lgain), (lup_h, lup), (qgain_h, qgain),
        (rout_h, wo.at[0:128]), (aout_h, wo.at[128:256]), (base_h, base), (far_h, far),
    ]
    copies = [pltpu.make_async_copy(s, d, in_sem.at[k]) for k, (s, d) in enumerate(loads)]
    for copy in copies:
        copy.start()

    copies[0].wait()
    copies[1].wait()
    own = tok[...].astype(F32)
    own = own * lax.rsqrt(jnp.mean(own * own, axis=1, keepdims=True) + EPS) * ngain[...]
    own_at = pl.multiple_of(32 * t, 32)
    xbuf[pl.ds(own_at, 32), :] = own.astype(BF16)

    pl.semaphore_wait(barrier, 6)

    def rows_of(xx, cc, half):
        return xbuf.at[pl.ds(pl.multiple_of(32 * tp_of(xx, cc) + 16 * half, 16), 16), :]

    mine = [rows_of(x, c, 0), rows_of(x, c, 1)]
    send(mine[0], mine[0], g_ssem.at[0], g_rsem.at[0], xup)
    send(mine[1], mine[1], g_ssem.at[3], g_rsem.at[3], xdn)
    send(mine[1], mine[1], g_ssem.at[1], g_rsem.at[1], xup)
    send(mine[0], mine[0], g_ssem.at[4], g_rsem.at[4], xdn)
    whole = xbuf.at[pl.ds(own_at, 32), :]
    send(whole, whole, d_ssem.at[0], d_rsem.at[0], partner)

    for copy in copies[2:5]:
        copy.wait()
    wa[:, 384:512] = wq[:, 0:128]
    wb[:, 0:128] = jnp.concatenate([wq[:, 128:192], wrk[...]], axis=1)
    wb[:, 128:256] = jnp.concatenate([wlat[...], jnp.zeros((D, 64), BF16)], axis=1)

    order = [
        (0, chip(-1), 0), (3, chip(1), 1), (1, chip(-1), 1), (4, chip(1), 0),
        (2, chip(2), 0), (5, chip(2), 1),
    ]
    for k, (sem, xx, half) in enumerate(order):
        piece = rows_of(xx, c, half)
        arrived(piece, g_rsem.at[sem])
        if sem == 0:
            send(piece, piece, g_ssem.at[2], g_rsem.at[2], xup)
        if sem == 3:
            send(piece, piece, g_ssem.at[5], g_rsem.at[5], xdn)
        send(piece, piece, d_ssem.at[1 + k], d_rsem.at[1 + k], partner)
    theirs = xbuf.at[pl.ds(pl.multiple_of(32 * tp_of(x, 1 - c), 32), 32), :]
    arrived(theirs, d_rsem.at[0])
    for k, (_, xx, half) in enumerate(order):
        arrived(rows_of(xx, 1 - c, half), d_rsem.at[1 + k])

    pb = dot(xbuf[...], wb[...]).astype(BF16)
    lat = pb[:, 128:192]
    latbuf[t] = jnp.concatenate([lat[0:128], lat[128:256]], axis=1)
    for k, peer in enumerate((xup, xfar, xdn)):
        send(latbuf.at[t], latbuf.at[t], l_ssem.at[k], l_rsem.at[k], peer)
    send(latbuf.at[t], latbuf.at[t], ld_ssem.at[0], ld_rsem.at[0], partner)

    for copy in copies[5:]:
        copy.wait()
    signal = dot(xbuf[...], wa[:, 0:256])
    recur = signal[:, 0:128].astype(BF16)
    halo_tx[...] = recur[240:256]
    send(halo_tx, halo_rx, h_sem.at[0], h_sem.at[1], zup)
    gate_s[...] = silu(signal[:, 128:256].astype(BF16).astype(F32))
    rest = dot(xbuf[...], wa[:, 256:512])
    agate_s[...] = silu(rest[:, 0:128].astype(BF16).astype(F32))

    far_row = far[pl.ds(z, 1), :]
    ca, sa, cb, sb = base[:, 0:128], base[:, 128:256], far_row[:, 0:128], far_row[:, 128:256]
    cosine, sine = ca * cb - sa * sb, sa * cb + ca * sb
    lane = lax.broadcasted_iota(jnp.int32, (TOK, 128), 1)
    first = lax.rem(lane, 64) < 32

    def rotated(v):
        swapped = jnp.where(first, -pltpu.roll(v, 96, 1), pltpu.roll(v, 32, 1))
        return v * cosine + swapped * sine

    q_nope = rest[:, 128:256].astype(BF16).astype(F32)
    qr_rk = pb[:, 0:128].astype(F32)
    q_half = jnp.where(lane < 64, qr_rk, 0.0)
    square = jnp.sum(q_nope * q_nope, axis=1, keepdims=True) + jnp.sum(
        q_half * q_half, axis=1, keepdims=True
    )
    scale = lax.rsqrt(square * (1.0 / 192.0) + EPS)
    qgain_rope = jnp.concatenate([qgain[:, 128:192], jnp.ones((1, 64), F32)], axis=1)
    q_nope = q_nope * scale * qgain[:, 0:128]
    turned = rotated(qr_rk * jnp.where(lane < 64, scale * qgain_rope, 1.0))
    zero64 = jnp.zeros((64, TOK), BF16)
    qn_s[...] = jnp.transpose(q_nope).astype(BF16)
    q_rope_t = jnp.transpose(turned)[0:64].astype(BF16)
    qlo_s[...] = jnp.concatenate([q_rope_t, zero64], axis=0)
    qhi_s[...] = jnp.concatenate([zero64, q_rope_t], axis=0)
    key_rope = turned[:, 64:128].astype(BF16)

    for k, o in enumerate((-1, -2, -3)):
        slot = latbuf.at[tp_of(chip(o), c)]
        arrived(slot, l_rsem.at[k])
        send(slot, slot, ld_ssem.at[1 + k], ld_rsem.at[1 + k], partner)
    arrived(latbuf.at[tp_of(x, 1 - c)], ld_rsem.at[0])
    for k, o in enumerate((-1, -2, -3)):
        arrived(latbuf.at[tp_of(chip(o), 1 - c)], ld_rsem.at[1 + k])
    packed = [latbuf[g] for g in range(8)]
    top = jnp.concatenate([v[:, 0:64] for v in packed], axis=1)
    bottom = jnp.concatenate([v[:, 64:128] for v in packed], axis=1)
    latent = jnp.concatenate([top, bottom], axis=0).astype(F32)
    latent = latent * lax.rsqrt(jnp.mean(latent * latent, axis=1, keepdims=True) + EPS) * lgain[...]
    kv = dot(latent.astype(BF16), lup[...])
    k_nope = kv[:, 0:128].astype(BF16)
    v_t = jnp.transpose(kv[:, 128:256]).astype(BF16)
    for h in range(2):
        r, p0 = 320 * h, 128 * h
        kvbuf[z, r : r + 128, :] = k_nope[p0 : p0 + 128]
        kvbuf[z, r + 128 : r + 256, :] = v_t[:, p0 : p0 + 128]
        kvbuf[z, r + 256 : r + 320, :] = jnp.concatenate(
            [key_rope[p0 : p0 + 64], key_rope[p0 + 64 : p0 + 128]], axis=1
        )

    def piece_at(slot, p):
        return kvbuf.at[slot, pl.ds(ROWS * p, ROWS), :]

    def forward(step, slot, direction, p):
        remote(
            piece_at(slot, p), piece_at(slot, p), kv_ssem.at[direction, step, p],
            kv_rsem.at[direction, step, p], zup if direction == 0 else zdn,
        ).start()

    def carry_on(step, slot, direction):
        remote(
            cbuf.at[slot], cbuf.at[slot], c_ssem.at[direction, step],
            c_rsem.at[direction, step], zup if direction == 0 else zdn,
        ).start()

    for p in range(PIECES):
        forward(0, z, 0, p)
        forward(0, z, 1, PIECES - 1 - p)

    row = lax.broadcasted_iota(jnp.int32, (TOK, 128), 0)
    arrived(halo_rx, h_sem.at[1])
    behind = jnp.where(z > 0, halo_rx[...].astype(F32), 0.0)
    recur = recur.astype(F32)
    conv_sum = None
    for tap in range(4):
        back = 3 - tap
        if back:
            moved = pltpu.roll(recur, back, 0)
            edge = pltpu.roll(behind, back, 0)
            edge = jnp.concatenate([edge[0:8], moved[8:TOK]], axis=0)
            term = jnp.where(row < back, edge, moved)
        else:
            term = recur
        term = conv[tap : tap + 1, :] * term
        conv_sum = term if conv_sum is None else conv_sum + term
    conv_out = conv_sum.astype(BF16)
    zb = jnp.zeros((64, 64), BF16)

    def diagonal(w):
        return jnp.concatenate(
            [jnp.concatenate([w[0], zb], axis=1), jnp.concatenate([zb, w[1]], axis=1)], axis=0
        )

    recur_rate = jax.nn.sigmoid(dot(conv_out, diagonal(rblk)))
    input_rate = jax.nn.sigmoid(dot(conv_out, diagonal(iblk)))
    shift = jnp.concatenate(
        [
            jnp.transpose(jnp.broadcast_to(dshift[:, p0 : p0 + 128], (128, 128)))
            for p0 in (0, 128)
        ],
        axis=0,
    )
    log_decay = -8.0 * recur_rate * drate[...] + shift
    a = jnp.exp(log_decay)
    b = jnp.sqrt(minus_expm1(2.0 * log_decay)) * input_rate * conv_out.astype(F32)
    for back in (1, 2, 4, 8, 16, 32, 64, 128):
        inside = row >= back
        a_before = jnp.where(inside, pltpu.roll(a, back, 0), 1.0)
        b_before = jnp.where(inside, pltpu.roll(b, back, 0), 0.0)
        b = a * b_before + b
        a = a * a_before
    a_s[...] = a
    b_s[...] = b
    cbuf[z] = jnp.concatenate([a[TOK - 1 : TOK], b[TOK - 1 : TOK], jnp.zeros((6, 128), F32)], axis=0)
    carry_on(0, z, 0)
    carry_on(0, z, 1)

    to_exp2 = float(192 ** -0.5 * np.log2(np.e))

    def scores(slot, h):
        r = 320 * h
        rope = kvbuf[slot, r + 256 : r + 320, :]
        s = dot(kvbuf[slot, r : r + 128, :], qn_s[...])
        s = s + jnp.concatenate([dot(rope, qlo_s[...]), dot(rope, qhi_s[...])], axis=0)
        return s * to_exp2

    def values(slot, h, weights):
        r = 320 * h
        return dot(kvbuf[slot, r + 128 : r + 256, :], weights.astype(BF16))

    key = lax.broadcasted_iota(jnp.int32, (128, TOK), 0)
    query = lax.broadcasted_iota(jnp.int32, (128, TOK), 1)
    s = [jnp.where(key + 128 * h <= query, scores(z, h), -jnp.inf) for h in range(2)]
    m = jnp.maximum(jnp.max(s[0], axis=0, keepdims=True), jnp.max(s[1], axis=0, keepdims=True))
    w = [jnp.exp2(v - m) for v in s]
    ml_s[0:1, :] = m
    ml_s[1:2, :] = jnp.sum(w[0] + w[1], axis=0, keepdims=True)
    acc_s[...] = values(z, 0, w[0]) + values(z, 1, w[1])

    def attend(slot):
        @pl.when(slot < z)
        def _():
            s = [scores(slot, h) for h in range(2)]
            old = ml_s[0:1, :]
            m = jnp.maximum(old, jnp.max(jnp.maximum(s[0], s[1]), axis=0, keepdims=True))
            w = [jnp.exp2(v - m) for v in s]
            rescale = jnp.exp2(old - m)
            ml_s[0:1, :] = m
            ml_s[1:2, :] = ml_s[1:2, :] * rescale + jnp.sum(w[0] + w[1], axis=0, keepdims=True)
            acc_s[...] = acc_s[...] * rescale + (values(slot, 0, w[0]) + values(slot, 1, w[1]))

    def step(s, up_pieces, dn_pieces, carries, before):
        up, dn = zat(-s), zat(s)
        for k in range(PIECES):
            p, q = k, PIECES - 1 - k
            arrived(piece_at(up, p), kv_rsem.at[0, s - 1, p])
            if p in up_pieces:
                forward(s, up, 0, p)
            arrived(piece_at(dn, q), kv_rsem.at[1, s - 1, q])
            if q in dn_pieces:
                forward(s, dn, 1, q)
            if before and k == 0:
                attend(zat(1 - s))
            if before and k == 1:
                attend(zat(s - 1))
        arrived(cbuf.at[up], c_rsem.at[0, s - 1])
        carry_on(s, up, 0)
        arrived(cbuf.at[dn], c_rsem.at[1, s - 1])
        if carries:
            carry_on(s, dn, 1)

    every = range(PIECES)
    step(1, every, every, True, False)

    def middle(s, _):
        step(s, every, every, True, True)
        return 0

    lax.fori_loop(2, 7, middle, 0)
    step(7, (0, 1), (2, 3), False, True)
    attend(zat(-7))
    attend(zat(7))
    last = zat(8)
    for p in (0, 1):
        arrived(piece_at(last, p), kv_rsem.at[0, 7, p])
        arrived(piece_at(last, 3 - p), kv_rsem.at[1, 7, 3 - p])
    arrived(cbuf.at[last], c_rsem.at[0, 7])
    attend(last)

    def onward(j, state):
        return jnp.where(j < z, cbuf[j, 0:1, :] * state + cbuf[j, 1:2, :], state)

    incoming = lax.fori_loop(0, NZ, onward, init[...])
    xrow[:, 0:128] = ((b_s[...] + a_s[...] * incoming) * gate_s[...]).astype(BF16)
    attended = jnp.transpose(acc_s[...] / ml_s[1:2, :])
    xrow[:, 128:256] = (attended * agate_s[...]).astype(BF16)

    offsets = (2, 1, -1, 0)
    for side, cc in enumerate((1 - c, c)):
        for k, o in enumerate(offsets):
            at = pl.multiple_of(32 * tp_of(chip(o), cc), 32)
            xcat[side, 32 * k : 32 * k + 32, :] = xrow[pl.ds(at, 32), :]
    d2d_tx[...] = dot(xcat[0], wo[...]).astype(BF16)
    for k in range(4):
        part = pl.ds(32 * k, 32)
        send(d2d_tx.at[part, :], d2d_rx.at[part, :], o_ssem.at[k], o_rsem.at[k], partner)
    psum[...] = dot(xcat[1], wo[...])

    def summed(k):
        part = slice(32 * k, 32 * k + 32)
        arrived(d2d_rx.at[pl.ds(32 * k, 32), :], o_rsem.at[k])
        return psum[part, :] + d2d_rx[part, :].astype(F32)

    def reduce_send(k, value, to):
        rtx[k] = value.astype(BF16)
        send(rtx.at[k], rrx.at[k], r_ssem.at[k], r_rsem.at[k], to)

    two = summed(0)
    reduce_send(0, two[:, 0:1024], xup)
    reduce_send(3, two[:, 1024:2048], xdn)
    above = summed(1)
    reduce_send(1, above[:, 1024:2048], xup)
    below = summed(2)
    reduce_send(4, below[:, 0:1024], xdn)
    arrived(rrx.at[0], r_rsem.at[0])
    reduce_send(2, above[:, 0:1024] + rrx[0].astype(F32), xup)
    arrived(rrx.at[3], r_rsem.at[3])
    reduce_send(5, below[:, 1024:2048] + rrx[3].astype(F32), xdn)
    here = summed(3)
    arrived(rrx.at[1], r_rsem.at[1])
    arrived(rrx.at[4], r_rsem.at[4])
    arrived(rrx.at[2], r_rsem.at[2])
    out_ref[:, 0:1024] = (
        here[:, 0:1024] + rrx[4].astype(F32) + rrx[2].astype(F32)
    ).astype(BF16)
    arrived(rrx.at[5], r_rsem.at[5])
    out_ref[:, 1024:2048] = (
        here[:, 1024:2048] + rrx[1].astype(F32) + rrx[5].astype(F32)
    ).astype(BF16)

    for copy in started:
        copy.wait_send()

    def drain(s, _):
        for direction in range(2):
            slot = zat(-s) if direction == 0 else zat(s)
            for p in range(PIECES):
                remote(
                    piece_at(slot, p), piece_at(slot, p), kv_ssem.at[direction, s, p],
                    kv_rsem.at[direction, s, p], partner,
                ).wait_send()
            remote(
                cbuf.at[slot], cbuf.at[slot], c_ssem.at[direction, s],
                c_rsem.at[direction, s], partner,
            ).wait_send()
        return 0

    lax.fori_loop(0, 7, drain, 0)
    for p in (0, 1):
        for direction, q in ((0, p), (1, 3 - p)):
            slot = zat(-7) if direction == 0 else zat(7)
            remote(
                piece_at(slot, q), piece_at(slot, q), kv_ssem.at[direction, 7, q],
                kv_rsem.at[direction, 7, q], partner,
            ).wait_send()
    remote(
        cbuf.at[zat(-7)], cbuf.at[zat(-7)], c_ssem.at[0, 7], c_rsem.at[0, 7], partner
    ).wait_send()


def body(
    tokens, norm_gain, recurrent_input, recurrent_gate, attention_gate, query_proj, latent_down,
    rope_key_down, conv_kernel, recurrence_gate_blocks, input_gate_blocks, decay_rate,
    decay_shift, initial_state, latent_gain, latent_up, query_gain, recurrent_output,
    attention_output,
):
    base, far = (jnp.asarray(v) for v in rotary_tables())

    def row(v):
        return v.reshape(1, -1)

    operands = (
        tokens, row(norm_gain), recurrent_input, recurrent_gate, attention_gate, query_proj,
        latent_down, rope_key_down, conv_kernel, recurrence_gate_blocks, input_gate_blocks,
        row(decay_rate), row(decay_shift), row(initial_state), row(latent_gain), latent_up,
        row(query_gain), recurrent_output, attention_output, base, far,
    )
    dma, vmem = pltpu.SemaphoreType.DMA, pltpu.VMEM
    scratch = [
        vmem((32, D), BF16), vmem((1, D), F32), vmem((D, 512), BF16), vmem((D, 256), BF16),
        vmem((D, 192), BF16), vmem((D, 64), BF16), vmem((D, 64), BF16), vmem((4, 128), F32),
        vmem((2, 64, 64), BF16), vmem((2, 64, 64), BF16), vmem((1, 128), F32),
        vmem((1, TOK), F32), vmem((1, 128), F32), vmem((1, 512), F32), vmem((512, 256), BF16),
        vmem((1, 192), F32), vmem((256, D), BF16), vmem((TOK, 256), F32), vmem((NZ, 256), F32),
        vmem((TOK, D), BF16), vmem((8, 128, 128), BF16), vmem((16, 128), BF16),
        vmem((16, 128), BF16), vmem((NZ, PIECES * ROWS, 128), BF16), vmem((NZ, 8, 128), F32),
        vmem((128, TOK), BF16), vmem((128, TOK), BF16), vmem((128, TOK), BF16),
        vmem((128, TOK), F32), vmem((8, TOK), F32), vmem((TOK, 128), F32),
        vmem((TOK, 128), F32), vmem((TOK, 128), F32), vmem((TOK, 128), F32),
        vmem((TOK, 256), BF16), vmem((2, 128, 256), BF16), vmem((128, D), BF16),
        vmem((128, D), BF16), vmem((128, D), F32), vmem((6, 32, 1024), BF16),
        vmem((6, 32, 1024), BF16),
        dma((len(operands),)), dma((6,)), dma((6,)), dma((7,)), dma((7,)), dma((3,)), dma((3,)),
        dma((4,)), dma((4,)), dma((2,)), dma((2, 8, PIECES)), dma((2, 8, PIECES)), dma((2, 8)),
        dma((2, 8)), dma((4,)), dma((4,)), dma((6,)), dma((6,)),
    ]
    return pl.pallas_call(
        kernel,
        out_shape=jax.ShapeDtypeStruct((32, D), BF16),
        in_specs=[pl.BlockSpec(memory_space=pl.ANY)] * len(operands),
        out_specs=pl.BlockSpec(memory_space=pltpu.VMEM),
        scratch_shapes=scratch,
        compiler_params=pltpu.CompilerParams(
            collective_id=0, has_side_effects=True, vmem_limit_bytes=56 * 2**20
        ),
    )(*operands)


def solution(mesh):
    return jax.shard_map(
        body,
        mesh=mesh,
        in_specs=(
            P(("fs", "sp", "tp"), None), P(), P(None, "tp"), P(None, "tp"), P(None, "tp"),
            P(None, "tp"), P(None, "tp"), P(), P(None, "tp"), P("tp", None, None),
            P("tp", None, None), P("tp"), P(("fs", "sp")), P(("fs", "tp")), P(), P(None, "tp"),
            P(), P("tp", None), P("tp", None),
        ),
        out_specs=P(("fs", "sp", "tp"), None),
        check_vma=False,
    )
```

```python
import functools

import jax
import jax.numpy as jnp
import numpy as np
from jax import lax
from jax.experimental import pallas as pl
from jax.experimental.pallas import tpu as pltpu
from jax.sharding import PartitionSpec as P

MESH = pl.DeviceIdType.MESH
EPS = 1e-06
THETA = 10000.0
F32, BF16 = jnp.float32, jnp.bfloat16
NZ, NX, TOK, D = 16, 4, 256, 2048
PIECES, ROWS = 6, 96
UP, DOWN = 8, 7
NT = (((1,), (1,)), ((), ()))


def dot(a, b):
    return jnp.dot(a, b, preferred_element_type=F32)


def silu(v):
    return v * jax.nn.sigmoid(v)


def minus_expm1(y):
    series = 1.0 + y * (1.0 / 8.0)
    for n in (7, 6, 5, 4, 3, 2):
        series = 1.0 + y * (1.0 / n) * series
    return jnp.where(y > -0.35, -y * series, 1.0 - jnp.exp(y))


def rotary_tables():
    inv = 1.0 / THETA ** (np.arange(0, 64, 2, dtype=np.float64) / 64)
    lanes = np.tile(inv, 4)

    def table(positions):
        angles = positions[:, None].astype(np.float64) * lanes[None]
        return np.concatenate([np.cos(angles), np.sin(angles)], 1).astype(np.float32)

    return table(np.arange(TOK)), table(TOK * np.arange(NZ))


def kernel(
    tok_h, ngain_h, rin_h, rgate_h, agate_h, wq_h, wlat_h, wrk_h, conv_h, rblk_h, iblk_h,
    drate_h, dshift_h, init_h, lgain_h, lup_h, qgain_h, rout_h, aout_h, base_h, far_h,
    out_ref,
    tok, ngain, wa, wb, wt, conv, rblk, iblk, drate, dshift, init, lgain, lup,
    qgain, wo, base, far,
    xbuf, latbuf, halo_tx, halo_rx, kvbuf, cbuf, qn_s, qlo_s, qhi_s, acc_s, ml_s,
    a_s, b_s, gate_s, agate_s, xrow, xcat, d2d_tx, d2d_rx, psum, rtx, rrx,
    in_sem, g_ssem, g_rsem, d_ssem, d_rsem, l_ssem, l_rsem, ld_ssem, ld_rsem, h_sem,
    kv_ssem, kv_rsem, s_ssem, s_rsem, c_ssem, c_rsem, o_ssem, o_rsem, r_ssem, r_rsem,
):
    z = lax.axis_index("sp")
    t = lax.axis_index("tp")
    x, c = lax.div(t, 2), lax.rem(t, 2)

    def chip(offset):
        return lax.rem(x + (offset + NX), NX)

    def tp_of(xx, cc):
        return 2 * xx + cc

    def zat(offset):
        return lax.rem(z + (offset + 2 * NZ), NZ)

    partner = {"tp": tp_of(x, 1 - c)}
    xup, xdn, xfar = ({"tp": tp_of(chip(o), c)} for o in (1, -1, 2))
    zup, zdn = {"sp": zat(1)}, {"sp": zat(-1)}
    started = []

    def remote(src, dst, ssem, rsem, to):
        return pltpu.make_async_remote_copy(
            src_ref=src, dst_ref=dst, send_sem=ssem, recv_sem=rsem, device_id=to,
            device_id_type=MESH,
        )

    def send(src, dst, ssem, rsem, to):
        copy = remote(src, dst, ssem, rsem, to)
        copy.start()
        started.append(copy)

    def arrived(dst, rsem, to=None):
        remote(dst, dst, rsem, rsem, partner).wait_recv()

    barrier = pltpu.get_barrier_semaphore()
    for peer in (partner, xup, xdn, xfar, zup, zdn):
        pl.semaphore_signal(barrier, inc=1, device_id=peer, device_id_type=MESH)

    loads = [
        (tok_h, tok), (ngain_h, ngain), (wq_h, wt.at[0:192]), (wrk_h, wt.at[192:256]),
        (wlat_h, wt.at[256:320]),
        (rin_h, wa.at[:, 0:128]), (rgate_h, wa.at[:, 128:256]), (agate_h, wa.at[:, 256:384]),
        (conv_h, conv), (rblk_h, rblk), (iblk_h, iblk), (drate_h, drate), (dshift_h, dshift),
        (init_h, init), (lgain_h, lgain), (lup_h, lup), (qgain_h, qgain),
        (rout_h, wo.at[0:128]), (aout_h, wo.at[128:256]), (base_h, base), (far_h, far),
    ]
    copies = [pltpu.make_async_copy(s, d, in_sem.at[k]) for k, (s, d) in enumerate(loads)]
    for copy in copies:
        copy.start()

    copies[0].wait()
    copies[1].wait()
    own = tok[...].astype(F32)
    own = own * lax.rsqrt(jnp.mean(own * own, axis=1, keepdims=True) + EPS) * ngain[...]
    own_at = pl.multiple_of(32 * t, 32)
    xbuf[pl.ds(own_at, 32), :] = own.astype(BF16)

    pl.semaphore_wait(barrier, 6)

    def rows_of(xx, cc, half):
        return xbuf.at[pl.ds(pl.multiple_of(32 * tp_of(xx, cc) + 16 * half, 16), 16), :]

    mine = [rows_of(x, c, 0), rows_of(x, c, 1)]
    send(mine[0], mine[0], g_ssem.at[0], g_rsem.at[0], xup)
    send(mine[1], mine[1], g_ssem.at[3], g_rsem.at[3], xdn)
    send(mine[1], mine[1], g_ssem.at[1], g_rsem.at[1], xup)
    send(mine[0], mine[0], g_ssem.at[4], g_rsem.at[4], xdn)
    whole = xbuf.at[pl.ds(own_at, 32), :]
    send(whole, whole, d_ssem.at[0], d_rsem.at[0], partner)

    for copy in copies[2:5]:
        copy.wait()
    wa[:, 384:512] = jnp.transpose(wt[0:128])
    wb[:, 0:128] = jnp.transpose(wt[128:256])
    wb[:, 128:256] = jnp.transpose(wt[256:384])

    order = [
        (0, chip(-1), 0), (3, chip(1), 1), (1, chip(-1), 1), (4, chip(1), 0),
        (2, chip(2), 0), (5, chip(2), 1),
    ]
    for k, (sem, xx, half) in enumerate(order):
        piece = rows_of(xx, c, half)
        arrived(piece, g_rsem.at[sem])
        if sem == 0:
            send(piece, piece, g_ssem.at[2], g_rsem.at[2], xup)
        if sem == 3:
            send(piece, piece, g_ssem.at[5], g_rsem.at[5], xdn)
        send(piece, piece, d_ssem.at[1 + k], d_rsem.at[1 + k], partner)
    theirs = xbuf.at[pl.ds(pl.multiple_of(32 * tp_of(x, 1 - c), 32), 32), :]
    arrived(theirs, d_rsem.at[0])
    for k, (_, xx, half) in enumerate(order):
        arrived(rows_of(xx, 1 - c, half), d_rsem.at[1 + k])

    pb = dot(xbuf[...], wb[...]).astype(BF16)
    lat = pb[:, 128:192]
    latbuf[t] = jnp.concatenate([lat[0:128], lat[128:256]], axis=1)
    for k, peer in enumerate((xup, xfar, xdn)):
        send(latbuf.at[t], latbuf.at[t], l_ssem.at[k], l_rsem.at[k], peer)
    send(latbuf.at[t], latbuf.at[t], ld_ssem.at[0], ld_rsem.at[0], partner)

    for copy in copies[5:]:
        copy.wait()
    signal = dot(xbuf[...], wa[:, 0:256])
    recur = signal[:, 0:128].astype(BF16)
    halo_tx[...] = recur[240:256]
    halo = remote(halo_tx, halo_rx, h_sem.at[0], h_sem.at[1], zup)
    pl.when(z < NZ - 1)(lambda: halo.start())
    gate_s[...] = silu(signal[:, 128:256].astype(BF16).astype(F32))
    rest = dot(xbuf[...], wa[:, 256:512])
    agate_s[...] = silu(rest[:, 0:128].astype(BF16).astype(F32))

    far_row = far[pl.ds(z, 1), :]
    ca, sa, cb, sb = base[:, 0:128], base[:, 128:256], far_row[:, 0:128], far_row[:, 128:256]
    cosine, sine = ca * cb - sa * sb, sa * cb + ca * sb
    lane = lax.broadcasted_iota(jnp.int32, (TOK, 128), 1)
    first = lax.rem(lane, 64) < 32

    def rotated(v):
        swapped = jnp.where(first, -pltpu.roll(v, 96, 1), pltpu.roll(v, 32, 1))
        return v * cosine + swapped * sine

    q_nope = rest[:, 128:256].astype(BF16).astype(F32)
    qr_rk = pb[:, 0:128].astype(F32)
    q_half = jnp.where(lane < 64, qr_rk, 0.0)
    square = jnp.sum(q_nope * q_nope, axis=1, keepdims=True) + jnp.sum(
        q_half * q_half, axis=1, keepdims=True
    )
    scale = lax.rsqrt(square * (1.0 / 192.0) + EPS)
    qgain_rope = jnp.concatenate([qgain[:, 128:192], jnp.ones((1, 64), F32)], axis=1)
    q_nope = q_nope * scale * qgain[:, 0:128]
    turned = rotated(qr_rk * jnp.where(lane < 64, scale * qgain_rope, 1.0))
    zero64 = jnp.zeros((64, TOK), BF16)
    qn_s[...] = jnp.transpose(q_nope).astype(BF16)
    q_rope_t = jnp.transpose(turned)[0:64].astype(BF16)
    qlo_s[...] = jnp.concatenate([q_rope_t, zero64], axis=0)
    qhi_s[...] = jnp.concatenate([zero64, q_rope_t], axis=0)
    key_rope = turned[:, 64:128].astype(BF16)

    for k, o in enumerate((-1, -2, -3)):
        slot = latbuf.at[tp_of(chip(o), c)]
        arrived(slot, l_rsem.at[k])
        send(slot, slot, ld_ssem.at[1 + k], ld_rsem.at[1 + k], partner)
    arrived(latbuf.at[tp_of(x, 1 - c)], ld_rsem.at[0])
    for k, o in enumerate((-1, -2, -3)):
        arrived(latbuf.at[tp_of(chip(o), 1 - c)], ld_rsem.at[1 + k])
    packed = [latbuf[g] for g in range(8)]
    top = jnp.concatenate([v[:, 0:64] for v in packed], axis=1)
    bottom = jnp.concatenate([v[:, 64:128] for v in packed], axis=1)
    latent = jnp.concatenate([top, bottom], axis=0).astype(F32)
    latent = latent * lax.rsqrt(jnp.mean(latent * latent, axis=1, keepdims=True) + EPS) * lgain[...]
    kv = dot(latent.astype(BF16), lup[...])
    k_nope = kv[:, 0:128].astype(BF16)
    v_t = jnp.transpose(kv[:, 128:256]).astype(BF16)
    for h in range(2):
        r, p0 = 64 + 256 * h, 128 * h
        kvbuf[z, r : r + 128, :] = k_nope[p0 : p0 + 128]
        kvbuf[z, r + 128 : r + 256, :] = v_t[:, p0 : p0 + 128]
        kvbuf[z, 576 * h : 576 * h + 64, :] = jnp.concatenate(
            [key_rope[p0 : p0 + 64], key_rope[p0 + 64 : p0 + 128]], axis=1
        )

    def piece_at(slot, k):
        p = k + c * (PIECES - 1 - 2 * k)
        return kvbuf.at[slot, pl.ds(pl.multiple_of(64 * c + ROWS * p, 16), ROWS), :]

    def forward(step, slot, direction, k):
        remote(
            piece_at(slot, k), piece_at(slot, k), kv_ssem.at[direction, step],
            kv_rsem.at[direction, step, k], zup if direction == 0 else zdn,
        ).start()

    def carry_on(step, slot, direction):
        remote(
            cbuf.at[slot], cbuf.at[slot], c_ssem.at[direction, step],
            c_rsem.at[direction, step], zup if direction == 0 else zdn,
        ).start()

    def shared(slot, core):
        return kvbuf.at[slot, pl.ds(pl.multiple_of(576 * core, 64), 64), :]

    def share(step, slot, direction):
        return remote(
            shared(slot, c), shared(slot, c), s_ssem.at[direction, step],
            s_rsem.at[direction, step], partner,
        )

    sends_up, sends_dn = z < NZ - 1, z < DOWN
    for k in range(PIECES):
        pl.when(sends_up)(lambda: forward(0, z, 0, k))
        pl.when(sends_dn)(lambda: forward(0, z, 1, k))

    row = lax.broadcasted_iota(jnp.int32, (TOK, 128), 0)
    pl.when(z > 0)(lambda: arrived(halo_rx, h_sem.at[1]))
    behind = jnp.where(z > 0, halo_rx[...].astype(F32), 0.0)
    recur = recur.astype(F32)
    conv_sum = None
    for tap in range(4):
        back = 3 - tap
        if back:
            moved = pltpu.roll(recur, back, 0)
            edge = pltpu.roll(behind, back, 0)
            edge = jnp.concatenate([edge[0:8], moved[8:TOK]], axis=0)
            term = jnp.where(row < back, edge, moved)
        else:
            term = recur
        term = conv[tap : tap + 1, :] * term
        conv_sum = term if conv_sum is None else conv_sum + term
    conv_out = conv_sum.astype(BF16)
    zb = jnp.zeros((64, 64), BF16)

    def diagonal(w):
        return jnp.concatenate(
            [jnp.concatenate([w[0], zb], axis=1), jnp.concatenate([zb, w[1]], axis=1)], axis=0
        )

    recur_rate = jax.nn.sigmoid(dot(conv_out, diagonal(rblk)))
    input_rate = jax.nn.sigmoid(dot(conv_out, diagonal(iblk)))
    shift = jnp.concatenate(
        [
            jnp.transpose(jnp.broadcast_to(dshift[:, p0 : p0 + 128], (128, 128)))
            for p0 in (0, 128)
        ],
        axis=0,
    )
    log_decay = -8.0 * recur_rate * drate[...] + shift
    a = jnp.exp(log_decay)
    b = jnp.sqrt(minus_expm1(2.0 * log_decay)) * input_rate * conv_out.astype(F32)
    for back in (1, 2, 4, 8, 16, 32, 64, 128):
        inside = row >= back
        a_before = jnp.where(inside, pltpu.roll(a, back, 0), 1.0)
        b_before = jnp.where(inside, pltpu.roll(b, back, 0), 0.0)
        b = a * b_before + b
        a = a * a_before
    a_s[...] = a
    b_s[...] = b
    cbuf[z] = jnp.concatenate([a[TOK - 1 : TOK], b[TOK - 1 : TOK], jnp.zeros((6, 128), F32)], axis=0)
    pl.when(sends_up)(lambda: carry_on(0, z, 0))
    pl.when(sends_dn)(lambda: carry_on(0, z, 1))

    to_exp2 = float(192 ** -0.5 * np.log2(np.e))

    def scores(slot, h):
        r = 64 + 256 * h
        rope = kvbuf[slot, 576 * h : 576 * h + 64, :]
        s = dot(kvbuf[slot, r : r + 128, :], qn_s[...])
        s = s + jnp.concatenate([dot(rope, qlo_s[...]), dot(rope, qhi_s[...])], axis=0)
        return s * to_exp2

    def values(slot, h, weights):
        r = 64 + 256 * h
        return dot(kvbuf[slot, r + 128 : r + 256, :], weights.astype(BF16))

    key = lax.broadcasted_iota(jnp.int32, (128, TOK), 0)
    query = lax.broadcasted_iota(jnp.int32, (128, TOK), 1)
    s = [jnp.where(key + 128 * h <= query, scores(z, h), -jnp.inf) for h in range(2)]
    m = jnp.maximum(jnp.max(s[0], axis=0, keepdims=True), jnp.max(s[1], axis=0, keepdims=True))
    w = [jnp.exp2(v - m) for v in s]
    ml_s[0:1, :] = m
    ml_s[1:2, :] = jnp.sum(w[0] + w[1], axis=0, keepdims=True)
    acc_s[...] = values(z, 0, w[0]) + values(z, 1, w[1])

    def attend(step, slot, direction):
        @pl.when(slot < z)
        def _():
            arrived(shared(slot, 1 - c), s_rsem.at[direction, step])
            s = [scores(slot, h) for h in range(2)]
            old = ml_s[0:1, :]
            m = jnp.maximum(old, jnp.max(jnp.maximum(s[0], s[1]), axis=0, keepdims=True))
            w = [jnp.exp2(v - m) for v in s]
            rescale = jnp.exp2(old - m)
            ml_s[0:1, :] = m
            ml_s[1:2, :] = ml_s[1:2, :] * rescale + jnp.sum(w[0] + w[1], axis=0, keepdims=True)
            acc_s[...] = acc_s[...] * rescale + (values(slot, 0, w[0]) + values(slot, 1, w[1]))

    def came_up(s):
        return zat(-s), s <= z

    def came_down(s):
        slot = zat(s)
        return slot, slot < DOWN

    def step(s, down, onward, before):
        up, has_up = came_up(s)
        dn, has_dn = came_down(s)
        for k in range(PIECES):

            @pl.when(has_up)
            def _():
                arrived(piece_at(up, k), kv_rsem.at[0, s - 1, k])
                if onward:
                    pl.when(sends_up)(lambda: forward(s, up, 0, k))
                if k == 0:
                    share(s - 1, up, 0).start()

            if down:

                @pl.when(has_dn)
                def _():
                    arrived(piece_at(dn, k), kv_rsem.at[1, s - 1, k])
                    if onward and down != "last":
                        forward(s, dn, 1, k)
                    if k == 0:
                        pl.when(dn < z)(lambda: share(s - 1, dn, 1).start())

            if before and k == 1:
                attend(s - 2, zat(1 - s), 0)
            if before and k == 3:
                attend(s - 2, zat(s - 1), 1)

        @pl.when(has_up)
        def _():
            arrived(cbuf.at[up], c_rsem.at[0, s - 1])
            if onward:
                pl.when(sends_up)(lambda: carry_on(s, up, 0))

        if down:

            @pl.when(has_dn)
            def _():
                arrived(cbuf.at[dn], c_rsem.at[1, s - 1])
                if onward and down != "last":
                    carry_on(s, dn, 1)

    step(1, True, True, False)

    def middle(s, _):
        step(s, True, True, True)
        return 0

    lax.fori_loop(2, DOWN, middle, 0)
    step(DOWN, "last", True, True)
    step(UP, False, False, True)
    attend(UP - 1, zat(-UP), 0)

    def onward(j, state):
        return jnp.where(j < z, cbuf[j, 0:1, :] * state + cbuf[j, 1:2, :], state)

    incoming = lax.fori_loop(0, NZ, onward, init[...])
    xrow[:, 0:128] = ((b_s[...] + a_s[...] * incoming) * gate_s[...]).astype(BF16)
    attended = jnp.transpose(acc_s[...] / ml_s[1:2, :])
    xrow[:, 128:256] = (attended * agate_s[...]).astype(BF16)

    offsets = (2, 1, -1, 0)
    for side, cc in enumerate((1 - c, c)):
        for k, o in enumerate(offsets):
            at = pl.multiple_of(32 * tp_of(chip(o), cc), 32)
            xcat[side, 32 * k : 32 * k + 32, :] = xrow[pl.ds(at, 32), :]
    d2d_tx[...] = dot(xcat[0], wo[...]).astype(BF16)
    for k in range(4):
        part = pl.ds(32 * k, 32)
        send(d2d_tx.at[part, :], d2d_rx.at[part, :], o_ssem.at[k], o_rsem.at[k], partner)
    psum[...] = dot(xcat[1], wo[...])

    def summed(k):
        part = slice(32 * k, 32 * k + 32)
        arrived(d2d_rx.at[pl.ds(32 * k, 32), :], o_rsem.at[k])
        return psum[part, :] + d2d_rx[part, :].astype(F32)

    def reduce_send(k, value, to):
        rtx[k] = value.astype(BF16)
        send(rtx.at[k], rrx.at[k], r_ssem.at[k], r_rsem.at[k], to)

    two = summed(0)
    reduce_send(0, two[:, 0:1024], xup)
    reduce_send(3, two[:, 1024:2048], xdn)
    above = summed(1)
    reduce_send(1, above[:, 1024:2048], xup)
    below = summed(2)
    reduce_send(4, below[:, 0:1024], xdn)
    arrived(rrx.at[0], r_rsem.at[0])
    reduce_send(2, above[:, 0:1024] + rrx[0].astype(F32), xup)
    arrived(rrx.at[3], r_rsem.at[3])
    reduce_send(5, below[:, 1024:2048] + rrx[3].astype(F32), xdn)
    here = summed(3)
    arrived(rrx.at[1], r_rsem.at[1])
    arrived(rrx.at[4], r_rsem.at[4])
    arrived(rrx.at[2], r_rsem.at[2])
    out_ref[:, 0:1024] = (
        here[:, 0:1024] + rrx[4].astype(F32) + rrx[2].astype(F32)
    ).astype(BF16)
    arrived(rrx.at[5], r_rsem.at[5])
    out_ref[:, 1024:2048] = (
        here[:, 1024:2048] + rrx[1].astype(F32) + rrx[5].astype(F32)
    ).astype(BF16)

    for copy in started:
        copy.wait_send()

    pl.when(z < NZ - 1)(lambda: halo.wait_send())

    def drain(s, _):
        for direction, (slot, has) in ((0, came_up(s)), (1, came_down(s))):
            goes = has & (sends_up if direction == 0 else s < DOWN)
            mine = kvbuf.at[slot, pl.ds(0, PIECES * ROWS), :]

            @pl.when(goes)
            def _():
                remote(
                    mine, mine, kv_ssem.at[direction, s], kv_rsem.at[direction, s, 0], partner
                ).wait_send()
                remote(
                    cbuf.at[slot], cbuf.at[slot], c_ssem.at[direction, s],
                    c_rsem.at[direction, s], partner,
                ).wait_send()

        return 0

    lax.fori_loop(0, UP, drain, 0)

    def drain_shared(s, _):
        for direction, slot in ((0, zat(-1 - s)), (1, zat(1 + s))):
            if direction == 0:
                pl.when(slot < z)(lambda: share(s, slot, 0).wait_send())
            else:
                pl.when((slot < z) & (s < DOWN))(lambda: share(s, slot, 1).wait_send())
        return 0

    lax.fori_loop(0, UP, drain_shared, 0)


def body(
    tokens, norm_gain, recurrent_input, recurrent_gate, attention_gate, query_proj, latent_down,
    rope_key_down, conv_kernel, recurrence_gate_blocks, input_gate_blocks, decay_rate,
    decay_shift, initial_state, latent_gain, latent_up, query_gain, recurrent_output,
    attention_output,
):
    base, far = (jnp.asarray(v) for v in rotary_tables())

    def row(v):
        return v.reshape(1, -1)

    operands = (
        tokens, row(norm_gain), recurrent_input, recurrent_gate, attention_gate, query_proj.T,
        latent_down.T, rope_key_down.T, conv_kernel, recurrence_gate_blocks, input_gate_blocks,
        row(decay_rate), row(decay_shift), row(initial_state), row(latent_gain), latent_up,
        row(query_gain), recurrent_output, attention_output, base, far,
    )
    dma, vmem = pltpu.SemaphoreType.DMA, pltpu.VMEM
    scratch = [
        vmem((32, D), BF16), vmem((1, D), F32), vmem((D, 512), BF16), vmem((D, 256), BF16),
        vmem((384, D), BF16), vmem((4, 128), F32),
        vmem((2, 64, 64), BF16), vmem((2, 64, 64), BF16), vmem((1, 128), F32),
        vmem((1, TOK), F32), vmem((1, 128), F32), vmem((1, 512), F32), vmem((512, 256), BF16),
        vmem((1, 192), F32), vmem((256, D), BF16), vmem((TOK, 256), F32), vmem((NZ, 256), F32),
        vmem((TOK, D), BF16), vmem((8, 128, 128), BF16), vmem((16, 128), BF16),
        vmem((16, 128), BF16), vmem((NZ, 640, 128), BF16), vmem((NZ, 8, 128), F32),
        vmem((128, TOK), BF16), vmem((128, TOK), BF16), vmem((128, TOK), BF16),
        vmem((128, TOK), F32), vmem((8, TOK), F32), vmem((TOK, 128), F32),
        vmem((TOK, 128), F32), vmem((TOK, 128), F32), vmem((TOK, 128), F32),
        vmem((TOK, 256), BF16), vmem((2, 128, 256), BF16), vmem((128, D), BF16),
        vmem((128, D), BF16), vmem((128, D), F32), vmem((6, 32, 1024), BF16),
        vmem((6, 32, 1024), BF16),
        dma((len(operands),)), dma((6,)), dma((6,)), dma((7,)), dma((7,)), dma((3,)), dma((3,)),
        dma((4,)), dma((4,)), dma((2,)), dma((2, 8)), dma((2, 8, PIECES)), dma((2, 8)), dma((2, 8)), dma((2, 8)),
        dma((2, 8)), dma((4,)), dma((4,)), dma((6,)), dma((6,)),
    ]
    return pl.pallas_call(
        kernel,
        out_shape=jax.ShapeDtypeStruct((32, D), BF16),
        in_specs=[pl.BlockSpec(memory_space=pl.ANY)] * len(operands),
        out_specs=pl.BlockSpec(memory_space=pltpu.VMEM),
        scratch_shapes=scratch,
        compiler_params=pltpu.CompilerParams(
            collective_id=0, has_side_effects=True, vmem_limit_bytes=56 * 2**20
        ),
    )(*operands)


def solution(mesh):
    return jax.shard_map(
        body,
        mesh=mesh,
        in_specs=(
            P(("fs", "sp", "tp"), None), P(), P(None, "tp"), P(None, "tp"), P(None, "tp"),
            P(None, "tp"), P(None, "tp"), P(), P(None, "tp"), P("tp", None, None),
            P("tp", None, None), P("tp"), P(("fs", "sp")), P(("fs", "tp")), P(), P(None, "tp"),
            P(), P("tp", None), P("tp", None),
        ),
        out_specs=P(("fs", "sp", "tp"), None),
        check_vma=False,
    )
```

```python
import functools

import jax
import jax.numpy as jnp
import numpy as np
from jax import lax
from jax.experimental import pallas as pl
from jax.experimental.pallas import tpu as pltpu
from jax.sharding import PartitionSpec as P

MESH = pl.DeviceIdType.MESH
EPS = 1e-06
THETA = 10000.0
F32, BF16 = jnp.float32, jnp.bfloat16
NZ, NX, TOK, D = 16, 4, 256, 2048
PIECES, HALF, ROWS = 6, 3, 96
UP, DOWN = 8, 7
NT = (((1,), (1,)), ((), ()))


def dot(a, b):
    return jnp.dot(a, b, preferred_element_type=F32)


def silu(v):
    return v * jax.nn.sigmoid(v)


def minus_expm1(y):
    series = 1.0 + y * (1.0 / 8.0)
    for n in (7, 6, 5, 4, 3, 2):
        series = 1.0 + y * (1.0 / n) * series
    return jnp.where(y > -0.35, -y * series, 1.0 - jnp.exp(y))


def rotary_tables():
    inv = 1.0 / THETA ** (np.arange(0, 64, 2, dtype=np.float64) / 64)
    lanes = np.tile(inv, 4)

    def table(positions):
        angles = positions[:, None].astype(np.float64) * lanes[None]
        return np.concatenate([np.cos(angles), np.sin(angles)], 1).astype(np.float32)

    return table(np.arange(TOK)), table(TOK * np.arange(NZ))


def kernel(
    tok_h, ngain_h, rin_h, rgate_h, agate_h, wq_h, wlat_h, wrk_h, conv_h, rblk_h, iblk_h,
    drate_h, dshift_h, init_h, lgain_h, lup_h, qgain_h, rout_h, aout_h, base_h, far_h,
    out_ref,
    tok, ngain, wa, wb, wt, conv, blocks, small, lup, qgain, wo, tables,
    xbuf, pbuf, latbuf, halo_tx, halo_rx, kvbuf, cbuf, qn_s, qlo_s, qhi_s, acc_s, ml_s,
    a_s, b_s, gate_s, agate_s, xrow, xcat, d2d_tx, d2d_rx, psum, rtx, rrx,
    in_sem, x_ssem, up_rsem, dn_rsem, d_rsem, l_ssem, l_rsem, ld_rsem, h_sem,
    up_ssem, dn_ssem, upkv_rsem, dnkv_rsem, s_ssem, s_rsem, c_rsem, o_ssem, o_rsem, r_ssem, r_rsem,
):
    z = lax.axis_index("sp")
    t = lax.axis_index("tp")
    x, c = lax.div(t, 2), lax.rem(t, 2)

    def chip(offset):
        return lax.rem(x + (offset + NX), NX)

    def tp_of(xx, cc):
        return 2 * xx + cc

    def zat(offset):
        return lax.rem(z + (offset + 2 * NZ), NZ)

    partner = {"tp": tp_of(x, 1 - c)}
    xup, xdn, xfar = ({"tp": tp_of(chip(o), c)} for o in (1, -1, 2))
    zup, zdn = {"sp": zat(1)}, {"sp": zat(-1)}
    across = [{"tp": tp_of(chip(o), 1 - c)} for o in (1, -1, 2)]

    def remote(src, dst, ssem, rsem, to):
        return pltpu.make_async_remote_copy(
            src_ref=src, dst_ref=dst, send_sem=ssem, recv_sem=rsem, device_id=to,
            device_id_type=MESH,
        )

    def send(src, dst, ssem, rsem, to):
        remote(src, dst, ssem, rsem, to).start()

    def arrived(dst, rsem):
        remote(dst, dst, rsem, rsem, partner).wait_recv()

    def sent(as_much, ssem):
        remote(as_much, as_much, ssem, ssem, partner).wait_send()

    barrier = pltpu.get_barrier_semaphore()
    for peer in (partner, xup, xdn, xfar, zup, zdn, *across):
        pl.semaphore_signal(barrier, inc=1, device_id=peer, device_id_type=MESH)

    loads = [
        (0, tok, [(tok_h, tok)]),
        (1, ngain, [(ngain_h, ngain)]),
        (2, wt.at[0:320], [(wq_h, wt.at[0:192]), (wrk_h, wt.at[192:256]), (wlat_h, wt.at[256:320])]),
        (3, wa.at[:, 0:384], [
            (rin_h, wa.at[:, 0:128]), (rgate_h, wa.at[:, 128:256]), (agate_h, wa.at[:, 256:384])
        ]),
        (4, conv, [(conv_h, conv)]),
        (5, blocks, [(rblk_h, blocks.at[0:2]), (iblk_h, blocks.at[2:4])]),
        (6, small, [
            (drate_h, small.at[0:1]), (init_h, small.at[1:2]), (dshift_h, small.at[2:4]),
            (lgain_h, small.at[4:8]),
        ]),
        (7, lup, [(lup_h, lup)]),
        (8, qgain, [(qgain_h, qgain)]),
        (9, wo, [(rout_h, wo.at[0:128]), (aout_h, wo.at[128:256])]),
        (10, tables, [(base_h, tables.at[0:TOK]), (far_h, tables.at[TOK : TOK + NZ])]),
    ]
    for k, _, copies in loads:
        for source, target in copies:
            pltpu.make_async_copy(source, target, in_sem.at[k]).start()

    def loaded(k):
        pltpu.make_async_copy(loads[k][1], loads[k][1], in_sem.at[k]).wait()

    loaded(0)
    loaded(1)
    own = tok[...].astype(F32)
    own = own * lax.rsqrt(jnp.mean(own * own, axis=1, keepdims=True) + EPS) * ngain[...]
    own_at = pl.multiple_of(32 * t, 32)
    xbuf[pl.ds(own_at, 32), :] = own.astype(BF16)

    pl.semaphore_wait(barrier, 9)

    def rows_of(xx, cc, half, columns=slice(None)):
        return xbuf.at[pl.ds(pl.multiple_of(32 * tp_of(xx, cc) + 16 * half, 16), 16), columns]

    left, right = slice(0, 1024), slice(1024, 2048)

    for k, part in enumerate((left, right)):
        send(rows_of(x, c, 0, part), rows_of(x, c, 0, part), x_ssem, up_rsem.at[k], xup)
        send(rows_of(x, c, 1, part), rows_of(x, c, 1, part), x_ssem, dn_rsem.at[k], xdn)
    send(rows_of(x, c, 1), rows_of(x, c, 1), x_ssem, up_rsem.at[2], xup)
    send(rows_of(x, c, 0), rows_of(x, c, 0), x_ssem, dn_rsem.at[2], xdn)
    whole = xbuf.at[pl.ds(own_at, 32), :]
    send(whole, whole, x_ssem, d_rsem.at[0], partner)

    loaded(2)
    wa[:, 384:512] = jnp.transpose(wt[0:128])
    wb[:, 0:128] = jnp.transpose(wt[128:256])
    wb[:, 128:256] = jnp.transpose(wt[256:384])

    for k, part in enumerate((left, right)):
        for piece, rsem, to in (
            (rows_of(chip(-1), c, 0, part), up_rsem, xup),
            (rows_of(chip(1), c, 1, part), dn_rsem, xdn),
        ):
            arrived(piece, rsem.at[k])
            send(piece, piece, x_ssem, rsem.at[3 + k], to)
            send(piece, piece, x_ssem, d_rsem.at[0], partner)
    for piece, rsem in ((rows_of(chip(-1), c, 1), up_rsem), (rows_of(chip(1), c, 0), dn_rsem)):
        arrived(piece, rsem.at[2])
        send(piece, piece, x_ssem, d_rsem.at[0], partner)
    arrived(xbuf.at[0:96, :], d_rsem.at[0])

    def segment(o):
        return pl.ds(pl.multiple_of(64 * chip(o), 64), 64)

    def project(offsets):
        rows = jnp.concatenate([xbuf[segment(o), :] for o in offsets], axis=0)
        out = dot(rows, wb[...]).astype(BF16)
        for k, o in enumerate(offsets):
            pbuf[segment(o), :] = out[64 * k : 64 * k + 64, 0:128]
            lat = out[64 * k : 64 * k + 64, 128:192]
            latbuf[t, 32 * o + 32 : 32 * o + 64, :] = jnp.concatenate([lat[0:32], lat[32:64]], axis=1)

    project((-1, 0, 1))
    early = latbuf.at[t, 0:96, :]
    for k, peer in enumerate((xup, xfar, xdn)):
        send(early, early, l_ssem, l_rsem.at[k], peer)
    send(early, early, l_ssem, ld_rsem, partner)
    for k, part in enumerate((left, right)):
        for half, rsem in ((0, up_rsem), (1, dn_rsem)):
            piece = rows_of(chip(2), c, half, part)
            arrived(piece, rsem.at[3 + k])
            send(piece, piece, x_ssem, d_rsem.at[1], partner)
    arrived(xbuf.at[0:32, :], d_rsem.at[1])
    project((2,))
    late = latbuf.at[t, 96:128, :]
    for peer in (xfar, across[2], xup, xdn, across[0], across[1], partner):
        send(late, late, l_ssem, l_rsem.at[3], peer)

    for k in range(3, 11):
        loaded(k)
    signal = dot(xbuf[...], wa[:, 0:256])
    recur = signal[:, 0:128].astype(BF16)
    halo_tx[...] = recur[240:256]
    halo = remote(halo_tx, halo_rx, h_sem.at[0], h_sem.at[1], zup)
    pl.when(z < NZ - 1)(lambda: halo.start())
    gate_s[...] = silu(signal[:, 128:256].astype(BF16).astype(F32))
    rest = dot(xbuf[...], wa[:, 256:512])
    agate_s[...] = silu(rest[:, 0:128].astype(BF16).astype(F32))

    base, far_row = tables[0:TOK, :], tables[pl.ds(TOK + z, 1), :]
    ca, sa, cb, sb = base[:, 0:128], base[:, 128:256], far_row[:, 0:128], far_row[:, 128:256]
    cosine, sine = ca * cb - sa * sb, sa * cb + ca * sb
    lane = lax.broadcasted_iota(jnp.int32, (TOK, 128), 1)
    first = lax.rem(lane, 64) < 32

    def rotated(v):
        swapped = jnp.where(first, -pltpu.roll(v, 96, 1), pltpu.roll(v, 32, 1))
        return v * cosine + swapped * sine

    q_nope = rest[:, 128:256].astype(BF16).astype(F32)
    qr_rk = pbuf[...].astype(F32)
    q_half = jnp.where(lane < 64, qr_rk, 0.0)
    square = jnp.sum(q_nope * q_nope, axis=1, keepdims=True) + jnp.sum(
        q_half * q_half, axis=1, keepdims=True
    )
    scale = lax.rsqrt(square * (1.0 / 192.0) + EPS)
    qgain_rope = jnp.concatenate([qgain[:, 128:192], jnp.ones((1, 64), F32)], axis=1)
    q_nope = q_nope * scale * qgain[:, 0:128]
    turned = rotated(qr_rk * jnp.where(lane < 64, scale * qgain_rope, 1.0))
    zero64 = jnp.zeros((64, TOK), BF16)
    qn_s[...] = jnp.transpose(q_nope).astype(BF16)
    q_rope_t = jnp.transpose(turned)[0:64].astype(BF16)
    qlo_s[...] = jnp.concatenate([q_rope_t, zero64], axis=0)
    qhi_s[...] = jnp.concatenate([zero64, q_rope_t], axis=0)
    key_rope = turned[:, 64:128].astype(BF16)

    for k, o in enumerate((-1, -2, -3)):
        slot = latbuf.at[tp_of(chip(o), c), 0:96, :]
        arrived(slot, l_rsem.at[k])
        send(slot, slot, l_ssem, ld_rsem, partner)
    arrived(latbuf.at[0:4, 0:96, :], ld_rsem)
    arrived(latbuf.at[0:7, 0:32, :], l_rsem.at[3])
    rows = []
    for g in range(4):
        for lanes in (slice(0, 64), slice(64, 128)):
            rows.append(
                jnp.concatenate(
                    [
                        latbuf[k, r : r + 32, lanes]
                        for k in range(8)
                        for r in (32 * ((g - k // 2 + 1) % 4),)
                    ],
                    axis=1,
                )
            )
    latent = jnp.concatenate(rows, axis=0).astype(F32)
    lgain = jnp.concatenate([small[k : k + 1, :] for k in range(4, 8)], axis=1)
    latent = latent * lax.rsqrt(jnp.mean(latent * latent, axis=1, keepdims=True) + EPS) * lgain
    kv = dot(latent.astype(BF16), lup[...])
    k_nope = kv[:, 0:128].astype(BF16)
    v_t = jnp.transpose(kv[:, 128:256]).astype(BF16)
    for h in range(2):
        r, p0 = 64 + 256 * h, 128 * h
        kvbuf[z, r : r + 128, :] = k_nope[p0 : p0 + 128]
        kvbuf[z, r + 128 : r + 256, :] = v_t[:, p0 : p0 + 128]
        kvbuf[z, 576 * h : 576 * h + 64, :] = jnp.concatenate(
            [key_rope[p0 : p0 + 64], key_rope[p0 + 64 : p0 + 128]], axis=1
        )

    def piece_at(slot, k):
        p = k + c * (PIECES - 1 - 2 * k)
        return kvbuf.at[slot, pl.ds(pl.multiple_of(64 * c + ROWS * p, 16), ROWS), :]

    def forward(step, slot, direction, k):
        piece = piece_at(slot, k)
        if direction == 0:
            send(piece, piece, up_ssem.at[step], upkv_rsem.at[step, k], zup)
        else:
            send(piece, piece, dn_ssem.at[step], dnkv_rsem.at[step, k], zdn)

    def carry_on(step, slot, direction):
        carry = cbuf.at[slot]
        ssem, to = (up_ssem, zup) if direction == 0 else (dn_ssem, zdn)
        send(carry, carry, ssem.at[step], c_rsem.at[direction, step], to)

    def shared(slot, core):
        return kvbuf.at[slot, pl.ds(pl.multiple_of(576 * core, 64), 64), :]

    def share(step, slot, direction):
        return remote(
            shared(slot, c), shared(slot, c), s_ssem.at[direction, step],
            s_rsem.at[direction, step], partner,
        )

    sends_up = z < NZ - 1
    for k in range(PIECES):
        pl.when(sends_up)(lambda: forward(0, z, 0, k))
        pl.when(z < (DOWN + 1 if k < HALF else DOWN))(lambda: forward(0, z, 1, PIECES - 1 - k))

    row = lax.broadcasted_iota(jnp.int32, (TOK, 128), 0)
    pl.when(z > 0)(lambda: arrived(halo_rx, h_sem.at[1]))
    behind = jnp.where(z > 0, halo_rx[...].astype(F32), 0.0)
    recur = recur.astype(F32)
    conv_sum = None
    for tap in range(4):
        back = 3 - tap
        if back:
            moved = pltpu.roll(recur, back, 0)
            edge = pltpu.roll(behind, back, 0)
            edge = jnp.concatenate([edge[0:8], moved[8:TOK]], axis=0)
            term = jnp.where(row < back, edge, moved)
        else:
            term = recur
        term = conv[tap : tap + 1, :] * term
        conv_sum = term if conv_sum is None else conv_sum + term
    conv_out = conv_sum.astype(BF16)
    zb = jnp.zeros((64, 64), BF16)

    def diagonal(w):
        return jnp.concatenate(
            [jnp.concatenate([w[0], zb], axis=1), jnp.concatenate([zb, w[1]], axis=1)], axis=0
        )

    recur_rate = jax.nn.sigmoid(dot(conv_out, diagonal(blocks[0:2])))
    input_rate = jax.nn.sigmoid(dot(conv_out, diagonal(blocks[2:4])))
    shift = jnp.concatenate(
        [
            jnp.transpose(jnp.broadcast_to(small[k : k + 1, :], (128, 128)))
            for k in (2, 3)
        ],
        axis=0,
    )
    log_decay = -8.0 * recur_rate * small[0:1, :] + shift
    a = jnp.exp(log_decay)
    b = jnp.sqrt(minus_expm1(2.0 * log_decay)) * input_rate * conv_out.astype(F32)
    for back in (1, 2, 4, 8, 16, 32, 64, 128):
        inside = row >= back
        a_before = jnp.where(inside, pltpu.roll(a, back, 0), 1.0)
        b_before = jnp.where(inside, pltpu.roll(b, back, 0), 0.0)
        b = a * b_before + b
        a = a * a_before
    a_s[...] = a
    b_s[...] = b
    cbuf[z] = jnp.concatenate([a[TOK - 1 : TOK], b[TOK - 1 : TOK], jnp.zeros((6, 128), F32)], axis=0)
    pl.when(sends_up)(lambda: carry_on(0, z, 0))
    pl.when(z < DOWN)(lambda: carry_on(0, z, 1))

    to_exp2 = float(192 ** -0.5 * np.log2(np.e))

    def scores(slot, h):
        r = 64 + 256 * h
        rope = kvbuf[slot, 576 * h : 576 * h + 64, :]
        s = dot(kvbuf[slot, r : r + 128, :], qn_s[...])
        s = s + jnp.concatenate([dot(rope, qlo_s[...]), dot(rope, qhi_s[...])], axis=0)
        return s * to_exp2

    def values(slot, h, weights):
        r = 64 + 256 * h
        return dot(kvbuf[slot, r + 128 : r + 256, :], weights.astype(BF16))

    key = lax.broadcasted_iota(jnp.int32, (128, TOK), 0)
    query = lax.broadcasted_iota(jnp.int32, (128, TOK), 1)
    s = [jnp.where(key + 128 * h <= query, scores(z, h), -jnp.inf) for h in range(2)]
    m = jnp.maximum(jnp.max(s[0], axis=0, keepdims=True), jnp.max(s[1], axis=0, keepdims=True))
    w = [jnp.exp2(v - m) for v in s]
    ml_s[0:1, :] = m
    ml_s[1:2, :] = jnp.sum(w[0] + w[1], axis=0, keepdims=True)
    acc_s[...] = values(z, 0, w[0]) + values(z, 1, w[1])

    def attend(step, slot, direction):
        @pl.when(slot < z)
        def _():
            arrived(shared(slot, 1 - c), s_rsem.at[direction, step])
            s = [scores(slot, h) for h in range(2)]
            old = ml_s[0:1, :]
            m = jnp.maximum(old, jnp.max(jnp.maximum(s[0], s[1]), axis=0, keepdims=True))
            w = [jnp.exp2(v - m) for v in s]
            rescale = jnp.exp2(old - m)
            ml_s[0:1, :] = m
            ml_s[1:2, :] = ml_s[1:2, :] * rescale + jnp.sum(w[0] + w[1], axis=0, keepdims=True)
            acc_s[...] = acc_s[...] * rescale + (values(slot, 0, w[0]) + values(slot, 1, w[1]))

    def step(s, before, last=False):
        up, dn = zat(-s), zat(s)
        has_up, has_dn = s <= z, dn < DOWN
        for k in range(PIECES):
            q = PIECES - 1 - k

            if k < HALF or not last:

                @pl.when(has_up)
                def _():
                    arrived(piece_at(up, k), upkv_rsem.at[s - 1, k])
                    if not last:
                        goes = sends_up & (s < DOWN) if k >= HALF else sends_up
                        pl.when(goes)(lambda: forward(s, up, 0, k))
                    if k == 0:
                        share(s - 1, up, 0).start()

                @pl.when((dn <= DOWN) if k < HALF else has_dn)
                def _():
                    arrived(piece_at(dn, q), dnkv_rsem.at[s - 1, q])
                    if not last:
                        if k < HALF:
                            forward(s, dn, 1, q)
                        else:
                            pl.when(s < DOWN)(lambda: forward(s, dn, 1, q))
                    if q == 0:
                        pl.when(dn < z)(lambda: share(s - 1, dn, 1).start())

            if before and k == 1:
                attend(s - 2, zat(1 - s), 0)
            if before and k == 3:
                attend(s - 2, zat(s - 1), 1)

        @pl.when(has_up)
        def _():
            arrived(cbuf.at[up], c_rsem.at[0, s - 1])
            if not last:
                pl.when(sends_up)(lambda: carry_on(s, up, 0))

        if not last:

            @pl.when(has_dn)
            def _():
                arrived(cbuf.at[dn], c_rsem.at[1, s - 1])
                pl.when(s < DOWN)(lambda: carry_on(s, dn, 1))

    offsets = (2, 1, -1, 0)

    def finish():
        def onward(j, state):
            return cbuf[j, 0:1, :] * state + cbuf[j, 1:2, :]

        incoming = lax.fori_loop(0, z, onward, small[1:2, :])
        xrow[:, 0:128] = ((b_s[...] + a_s[...] * incoming) * gate_s[...]).astype(BF16)
        attended = jnp.transpose(acc_s[...] / ml_s[1:2, :])
        xrow[:, 128:256] = (attended * agate_s[...]).astype(BF16)
        for side, cc in enumerate((1 - c, c)):
            for k, o in enumerate(offsets):
                at = pl.multiple_of(32 * tp_of(chip(o), cc), 32)
                xcat[side, 32 * k : 32 * k + 32, :] = xrow[pl.ds(at, 32), :]
        d2d_tx[...] = dot(xcat[0], wo[...]).astype(BF16)
        for k in range(4):
            part = slice(32 * k, 32 * k + 32)
            send(d2d_tx.at[part, :], d2d_rx.at[part, :], o_ssem, o_rsem.at[k], partner)
        psum[...] = dot(xcat[1], wo[...])

    def ship(k, value, to):
        width = value.shape[1]
        rtx[k, :, 0:width] = value.astype(BF16)
        send(rtx.at[k, :, 0:width], rrx.at[k, :, 0:width], r_ssem, r_rsem.at[k], to)

    def landed(k, width=512):
        arrived(rrx.at[k, :, 0:width], r_rsem.at[k])
        return rrx[k, :, 0:width].astype(F32)

    def add_partner(k):
        part = slice(32 * k, 32 * k + 32)
        arrived(d2d_rx.at[part, :], o_rsem.at[k])
        both = psum[part, :] + d2d_rx[part, :].astype(F32)
        psum[part, :] = both
        return both

    def reduce_first():
        two = add_partner(0)
        ship(0, two[:, 0:512], xup)
        ship(5, two[:, 1024:1536], xdn)
        ship(1, two[:, 512:1024], xup)
        ship(6, two[:, 1536:2048], xdn)
        ship(2, add_partner(1)[:, 1024:2048], xup)
        ship(7, add_partner(2)[:, 0:1024], xdn)

    def reduce_second():
        for k in range(2):
            at = 512 * k
            ship(3 + k, psum[32:64, at : at + 512] + landed(k), xup)
            ship(8 + k, psum[64:96, 1024 + at : 1536 + at] + landed(5 + k), xdn)

    def reduce_last():
        add_partner(3)
        direct = (landed(7, 1024), landed(2, 1024))
        for k in range(2):
            for side in range(2):
                at = 1024 * side + 512 * k
                total = psum[96:128, at : at + 512] + direct[side][:, 512 * k : 512 * k + 512]
                out_ref[:, at : at + 512] = (total + landed((3, 8)[side] + k)).astype(BF16)

    def between(when, stage):
        pl.when((z < 2) & when)(stage)

    step(1, False)

    def middle(s, _):
        step(s, True)
        between(s == 2, finish)
        between(s == 3, reduce_first)
        between(s == 4, reduce_second)
        between(s == 5, reduce_last)
        return 0

    lax.fori_loop(2, UP, middle, 0)
    step(UP, True, last=True)
    attend(UP - 1, zat(-UP), 0)

    @pl.when(z >= 2)
    def _():
        finish()
        reduce_first()
        reduce_second()
        reduce_last()


    @pl.when(sends_up)
    def _():
        sent(halo_tx, h_sem.at[0])

    def drain(s, _):
        dn = zat(s)
        first, full = pl.ds(0, HALF * ROWS), pl.ds(0, PIECES * ROWS + 16)

        @pl.when(sends_up & (s <= z))
        def _():
            pl.when(s < DOWN)(lambda: sent(kvbuf.at[0, full, :], up_ssem.at[s]))
            pl.when(s == DOWN)(
                lambda: sent(kvbuf.at[0, pl.ds(0, HALF * ROWS + 16), :], up_ssem.at[s])
            )

        whole = (dn < DOWN) & (s < DOWN)
        pl.when(whole)(lambda: sent(kvbuf.at[0, full, :], dn_ssem.at[s]))
        pl.when((dn <= DOWN) & jnp.logical_not(whole))(
            lambda: sent(kvbuf.at[0, first, :], dn_ssem.at[s])
        )
        pl.when(zat(-1 - s) < z)(lambda: sent(shared(0, c), s_ssem.at[0, s]))
        pl.when((zat(1 + s) < z) & (s < DOWN))(lambda: sent(shared(0, c), s_ssem.at[1, s]))
        return 0

    lax.fori_loop(0, UP, drain, 0)
    sent(xbuf.at[0:224, :], x_ssem)
    sent(latbuf.at[0:7, :, :], l_ssem)
    sent(d2d_tx, o_ssem)
    sent(rtx.at[0:6, :, :], r_ssem)


def body(
    tokens, norm_gain, recurrent_input, recurrent_gate, attention_gate, query_proj, latent_down,
    rope_key_down, conv_kernel, recurrence_gate_blocks, input_gate_blocks, decay_rate,
    decay_shift, initial_state, latent_gain, latent_up, query_gain, recurrent_output,
    attention_output,
):
    base, far = (jnp.asarray(v) for v in rotary_tables())

    def row(v):
        return v.reshape(1, -1)

    operands = (
        tokens, row(norm_gain), recurrent_input, recurrent_gate, attention_gate, query_proj.T,
        latent_down.T, rope_key_down.T, conv_kernel, recurrence_gate_blocks, input_gate_blocks,
        row(decay_rate), decay_shift.reshape(2, 128), row(initial_state),
        latent_gain.reshape(4, 128), latent_up,
        row(query_gain), recurrent_output, attention_output, base, far,
    )
    dma, vmem = pltpu.SemaphoreType.DMA, pltpu.VMEM
    scratch = [
        vmem((32, D), BF16), vmem((1, D), F32), vmem((D, 512), BF16), vmem((D, 256), BF16),
        vmem((384, D), BF16), vmem((4, 128), F32), vmem((4, 64, 64), BF16), vmem((8, 128), F32),
        vmem((512, 256), BF16), vmem((1, 192), F32), vmem((256, D), BF16),
        vmem((TOK + NZ, 256), F32),
        vmem((TOK, D), BF16), vmem((TOK, 128), BF16), vmem((8, 128, 128), BF16),
        vmem((16, 128), BF16), vmem((16, 128), BF16), vmem((NZ, 640, 128), BF16),
        vmem((NZ, 8, 128), F32), vmem((128, TOK), BF16), vmem((128, TOK), BF16),
        vmem((128, TOK), BF16), vmem((128, TOK), F32), vmem((8, TOK), F32),
        vmem((TOK, 128), F32), vmem((TOK, 128), F32), vmem((TOK, 128), F32),
        vmem((TOK, 128), F32), vmem((TOK, 256), BF16), vmem((2, 128, 256), BF16),
        vmem((128, D), BF16), vmem((128, D), BF16), vmem((128, D), F32),
        vmem((10, 32, 1024), BF16), vmem((10, 32, 1024), BF16),
        dma((11,)), dma(()), dma((5,)), dma((5,)), dma((2,)), dma(()), dma((4,)), dma(()),
        dma((2,)), dma((8,)), dma((8,)), dma((8, PIECES)), dma((8, PIECES)), dma((2, 8)),
        dma((2, 8)), dma((2, 8)), dma(()), dma((4,)), dma(()), dma((10,)),
    ]
    return pl.pallas_call(
        kernel,
        out_shape=pltpu.VMEM((32, D), BF16),
        in_specs=[pl.BlockSpec(memory_space=pl.ANY)] * len(operands),
        scratch_shapes=scratch,
        compiler_params=pltpu.CompilerParams(
            collective_id=0, has_side_effects=True, vmem_limit_bytes=56 * 2**20
        ),
    )(*operands)


def solution(mesh):
    return jax.shard_map(
        body,
        mesh=mesh,
        in_specs=(
            P(("fs", "sp", "tp"), None), P(), P(None, "tp"), P(None, "tp"), P(None, "tp"),
            P(None, "tp"), P(None, "tp"), P(), P(None, "tp"), P("tp", None, None),
            P("tp", None, None), P("tp"), P(("fs", "sp")), P(("fs", "tp")), P(), P(None, "tp"),
            P(), P("tp", None), P("tp", None),
        ),
        out_specs=P(("fs", "sp", "tp"), None),
        check_vma=False,
    )
```

```python
import functools

import jax
import jax.numpy as jnp
import numpy as np
from jax import lax
from jax.experimental import pallas as pl
from jax.experimental.pallas import tpu as pltpu
from jax.sharding import PartitionSpec as P

MESH = pl.DeviceIdType.MESH
EPS = 1e-06
THETA = 10000.0
F32, BF16 = jnp.float32, jnp.bfloat16
NZ, NX, TOK, D = 16, 4, 256, 2048
PARTS = ((0, 96), (96, 80), (176, 80), (256, 96), (352, 80), (432, 80))
PIECES, HALF = 6, 3
UP, DOWN = 8, 7
NT = (((1,), (1,)), ((), ()))


def dot(a, b):
    return jnp.dot(a, b, preferred_element_type=F32)


def silu(v):
    return v * jax.nn.sigmoid(v)


def minus_expm1(y):
    series = 1.0 + y * (1.0 / 8.0)
    for n in (7, 6, 5, 4, 3, 2):
        series = 1.0 + y * (1.0 / n) * series
    return jnp.where(y > -0.35, -y * series, 1.0 - jnp.exp(y))


def rotary_tables():
    inv = 1.0 / THETA ** (np.arange(0, 64, 2, dtype=np.float64) / 64)
    lanes = np.tile(inv, 4)

    def table(positions):
        angles = positions[:, None].astype(np.float64) * lanes[None]
        return np.concatenate([np.cos(angles), np.sin(angles)], 1).astype(np.float32)

    return table(np.arange(TOK)), table(TOK * np.arange(NZ))


def kernel(
    tok_h, ngain_h, rin_h, rgate_h, agate_h, wq_h, wlat_h, wrk_h, conv_h, rblk_h, iblk_h,
    drate_h, dshift_h, init_h, lgain_h, lup_h, qgain_h, rout_h, aout_h, base_h, far_h,
    out_ref,
    tok, ngain, wa, wb, wt, conv, blocks, small, lup, qgain, wo, tables,
    xbuf, pbuf, latbuf, halo_tx, halo_rx, kvbuf, cbuf, qn_s, qlo_s, qhi_s, acc_s, ml_s,
    a_s, b_s, gate_s, agate_s, xrow, xcat, d2d_tx, d2d_rx, psum, rtx, rrx, ropebuf,
    in_sem, x_ssem, up_rsem, dn_rsem, d_rsem, l_ssem, l_rsem, ld_rsem, h_sem,
    up_ssem, dn_ssem, upkv_rsem, dnkv_rsem, s_ssem, s_rsem, rr_sem, c_ssem, c_rsem, o_ssem, o_rsem, r_ssem, r_rsem,
):
    z = lax.axis_index("sp")
    t = lax.axis_index("tp")
    x, c = lax.div(t, 2), lax.rem(t, 2)

    def chip(offset):
        return lax.rem(x + (offset + NX), NX)

    def tp_of(xx, cc):
        return 2 * xx + cc

    def zat(offset):
        return lax.rem(z + (offset + 2 * NZ), NZ)

    partner = {"tp": tp_of(x, 1 - c)}
    xup, xdn, xfar = ({"tp": tp_of(chip(o), c)} for o in (1, -1, 2))
    zup, zdn = {"sp": zat(1)}, {"sp": zat(-1)}
    across = [{"tp": tp_of(chip(o), 1 - c)} for o in (1, -1, 2)]

    def remote(src, dst, ssem, rsem, to):
        return pltpu.make_async_remote_copy(
            src_ref=src, dst_ref=dst, send_sem=ssem, recv_sem=rsem, device_id=to,
            device_id_type=MESH,
        )

    def send(src, dst, ssem, rsem, to):
        remote(src, dst, ssem, rsem, to).start()

    def arrived(dst, rsem):
        remote(dst, dst, rsem, rsem, partner).wait_recv()

    def sent(as_much, ssem):
        remote(as_much, as_much, ssem, ssem, partner).wait_send()

    barrier = pltpu.get_barrier_semaphore()
    for peer in (partner, xup, xdn, xfar, zup, zdn, *across):
        pl.semaphore_signal(barrier, inc=1, device_id=peer, device_id_type=MESH)

    loads = [
        (0, tok, [(tok_h, tok)]),
        (1, ngain, [(ngain_h, ngain)]),
        (2, wt.at[0:320], [(wq_h, wt.at[0:192]), (wrk_h, wt.at[192:256]), (wlat_h, wt.at[256:320])]),
        (3, wa.at[:, 0:384], [
            (rin_h, wa.at[:, 0:128]), (rgate_h, wa.at[:, 128:256]), (agate_h, wa.at[:, 256:384])
        ]),
        (4, conv, [(conv_h, conv)]),
        (5, blocks, [(rblk_h, blocks.at[0:2]), (iblk_h, blocks.at[2:4])]),
        (6, small, [
            (drate_h, small.at[0:1]), (init_h, small.at[1:2]), (dshift_h, small.at[2:4]),
            (lgain_h, small.at[4:8]),
        ]),
        (7, lup, [(lup_h, lup)]),
        (8, qgain, [(qgain_h, qgain)]),
        (9, wo, [(rout_h, wo.at[0:128]), (aout_h, wo.at[128:256])]),
        (10, tables, [(base_h, tables.at[0:TOK]), (far_h, tables.at[TOK : TOK + NZ])]),
    ]
    for k, _, copies in loads:
        for source, target in copies:
            pltpu.make_async_copy(source, target, in_sem.at[k]).start()

    def loaded(k):
        pltpu.make_async_copy(loads[k][1], loads[k][1], in_sem.at[k]).wait()

    loaded(0)
    loaded(1)
    own = tok[...].astype(F32)
    own = own * lax.rsqrt(jnp.mean(own * own, axis=1, keepdims=True) + EPS) * ngain[...]
    own_at = pl.multiple_of(32 * t, 32)
    xbuf[pl.ds(own_at, 32), :] = own.astype(BF16)

    pl.semaphore_wait(barrier, 9)

    def rows_of(xx, cc, half, columns=slice(None)):
        return xbuf.at[pl.ds(pl.multiple_of(32 * tp_of(xx, cc) + 16 * half, 16), 16), columns]

    left, right = slice(0, 1024), slice(1024, 2048)

    for k, part in enumerate((left, right)):
        send(rows_of(x, c, 0, part), rows_of(x, c, 0, part), x_ssem, up_rsem.at[k], xup)
        send(rows_of(x, c, 1, part), rows_of(x, c, 1, part), x_ssem, dn_rsem.at[k], xdn)
    send(rows_of(x, c, 1), rows_of(x, c, 1), x_ssem, up_rsem.at[2], xup)
    send(rows_of(x, c, 0), rows_of(x, c, 0), x_ssem, dn_rsem.at[2], xdn)
    whole = xbuf.at[pl.ds(own_at, 32), :]
    send(whole, whole, x_ssem, d_rsem.at[0], partner)

    loaded(2)
    wa[:, 384:512] = jnp.transpose(wt[0:128])
    wb[:, 0:128] = jnp.transpose(wt[128:256])
    wb[:, 128:256] = jnp.transpose(wt[256:384])

    for k, part in enumerate((left, right)):
        for piece, rsem, to in (
            (rows_of(chip(-1), c, 0, part), up_rsem, xup),
            (rows_of(chip(1), c, 1, part), dn_rsem, xdn),
        ):
            arrived(piece, rsem.at[k])
            send(piece, piece, x_ssem, rsem.at[3 + k], to)
            send(piece, piece, x_ssem, d_rsem.at[0], partner)
    for piece, rsem in ((rows_of(chip(-1), c, 1), up_rsem), (rows_of(chip(1), c, 0), dn_rsem)):
        arrived(piece, rsem.at[2])
        send(piece, piece, x_ssem, d_rsem.at[0], partner)
    arrived(xbuf.at[0:96, :], d_rsem.at[0])

    def segment(o):
        return pl.ds(pl.multiple_of(64 * chip(o), 64), 64)

    def project(offsets):
        rows = jnp.concatenate([xbuf[segment(o), :] for o in offsets], axis=0)
        out = dot(rows, wb[...]).astype(BF16)
        for k, o in enumerate(offsets):
            pbuf[segment(o), :] = out[64 * k : 64 * k + 64, 0:128]
            lat = out[64 * k : 64 * k + 64, 128:192]
            latbuf[t, 32 * o + 32 : 32 * o + 64, :] = jnp.concatenate([lat[0:32], lat[32:64]], axis=1)

    project((-1, 0, 1))
    early = latbuf.at[t, 0:96, :]
    for k, peer in enumerate((xup, xfar, xdn)):
        send(early, early, l_ssem, l_rsem.at[k], peer)
    send(early, early, l_ssem, ld_rsem, partner)
    for k, part in enumerate((left, right)):
        for half, rsem in ((0, up_rsem), (1, dn_rsem)):
            piece = rows_of(chip(2), c, half, part)
            arrived(piece, rsem.at[3 + k])
            send(piece, piece, x_ssem, d_rsem.at[1], partner)
    arrived(xbuf.at[0:32, :], d_rsem.at[1])
    project((2,))
    late = latbuf.at[t, 96:128, :]
    for peer in (xfar, across[2], xup, xdn, across[0], across[1], partner):
        send(late, late, l_ssem, l_rsem.at[3], peer)

    for k in range(3, 11):
        loaded(k)
    signal = dot(xbuf[...], wa[:, 0:256])
    recur = signal[:, 0:128].astype(BF16)
    halo_tx[...] = recur[240:256]
    halo = remote(halo_tx, halo_rx, h_sem.at[0], h_sem.at[1], zup)
    pl.when(z < NZ - 1)(lambda: halo.start())
    gate_s[...] = silu(signal[:, 128:256].astype(BF16).astype(F32))
    rest = dot(xbuf[...], wa[:, 256:512])
    agate_s[...] = silu(rest[:, 0:128].astype(BF16).astype(F32))

    sends_up = z < NZ - 1

    def piece_at(slot, k):
        return kvbuf.at[slot, pl.ds(*PARTS[k]), :]

    def onward(direction, what, step, rsem):
        if direction == 0:
            send(what, what, up_ssem.at[step], rsem, zup)
        else:
            send(what, what, dn_ssem.at[step], rsem, zdn)

    def forward(step, slot, direction, k):
        rsem = upkv_rsem if direction == 0 else dnkv_rsem
        onward(direction, piece_at(slot, k), step, rsem.at[step, k])

    def carry_on(step, slot, direction):
        carry = cbuf.at[slot]
        rsem, to = c_rsem.at[direction, step], (zup, zdn)[direction]
        send(carry, carry, c_ssem.at[direction, step], rsem, to)

    own_sixteenth = pl.ds(pl.multiple_of(16 * t, 16), 16)

    def rope_on(step, slot, direction):
        onward(direction, ropebuf.at[slot, own_sixteenth, :], step, rr_sem.at[direction, step])

    def share(step, slot, direction):
        mine = ropebuf.at[slot, own_sixteenth, :]
        for peer in (xfar, across[2], xup, xdn, across[0], across[1], partner):
            send(mine, mine, s_ssem.at[direction, step], s_rsem.at[direction, step], peer)

    def rope_step(s):
        up, dn = zat(-s), zat(s)

        @pl.when((s <= z) & (s <= UP))
        def _():
            arrived(ropebuf.at[up, own_sixteenth, :], rr_sem.at[0, s - 1])
            pl.when(sends_up & (s < UP))(lambda: rope_on(s, up, 0))
            share(s - 1, up, 0)

        @pl.when((dn < DOWN) & (s <= DOWN))
        def _():
            arrived(ropebuf.at[dn, own_sixteenth, :], rr_sem.at[1, s - 1])
            pl.when(s < DOWN)(lambda: rope_on(s, dn, 1))
            pl.when(dn < z)(lambda: share(s - 1, dn, 1))

    base, far_row = tables[0:TOK, :], tables[pl.ds(TOK + z, 1), :]
    ca, sa, cb, sb = base[:, 0:128], base[:, 128:256], far_row[:, 0:128], far_row[:, 128:256]
    cosine, sine = ca * cb - sa * sb, sa * cb + ca * sb
    lane = lax.broadcasted_iota(jnp.int32, (TOK, 128), 1)
    first = lax.rem(lane, 64) < 32

    def rotated(v):
        swapped = jnp.where(first, -pltpu.roll(v, 96, 1), pltpu.roll(v, 32, 1))
        return v * cosine + swapped * sine

    q_nope = rest[:, 128:256].astype(BF16).astype(F32)
    qr_rk = pbuf[...].astype(F32)
    q_half = jnp.where(lane < 64, qr_rk, 0.0)
    square = jnp.sum(q_nope * q_nope, axis=1, keepdims=True) + jnp.sum(
        q_half * q_half, axis=1, keepdims=True
    )
    scale = lax.rsqrt(square * (1.0 / 192.0) + EPS)
    qgain_rope = jnp.concatenate([qgain[:, 128:192], jnp.ones((1, 64), F32)], axis=1)
    q_nope = q_nope * scale * qgain[:, 0:128]
    turned = rotated(qr_rk * jnp.where(lane < 64, scale * qgain_rope, 1.0))
    zero64 = jnp.zeros((64, TOK), BF16)
    qn_s[...] = jnp.transpose(q_nope).astype(BF16)
    q_rope_t = jnp.transpose(turned)[0:64].astype(BF16)
    qlo_s[...] = jnp.concatenate([q_rope_t, zero64], axis=0)
    qhi_s[...] = jnp.concatenate([zero64, q_rope_t], axis=0)
    key_rope = turned[:, 64:128].astype(BF16)
    for h in range(2):
        p0 = 128 * h
        ropebuf[z, 64 * h : 64 * h + 64, :] = jnp.concatenate(
            [key_rope[p0 : p0 + 64], key_rope[p0 + 64 : p0 + 128]], axis=1
        )
    pl.when(sends_up)(lambda: rope_on(0, z, 0))
    pl.when(z < DOWN)(lambda: rope_on(0, z, 1))

    for k, o in enumerate((-1, -2, -3)):
        slot = latbuf.at[tp_of(chip(o), c), 0:96, :]
        arrived(slot, l_rsem.at[k])
        send(slot, slot, l_ssem, ld_rsem, partner)
    arrived(latbuf.at[0:4, 0:96, :], ld_rsem)
    arrived(latbuf.at[0:7, 0:32, :], l_rsem.at[3])
    rows = []
    for g in range(4):
        for lanes in (slice(0, 64), slice(64, 128)):
            rows.append(
                jnp.concatenate(
                    [
                        latbuf[k, r : r + 32, lanes]
                        for k in range(8)
                        for r in (32 * ((g - k // 2 + 1) % 4),)
                    ],
                    axis=1,
                )
            )
    latent = jnp.concatenate(rows, axis=0).astype(F32)
    lgain = jnp.concatenate([small[k : k + 1, :] for k in range(4, 8)], axis=1)
    latent = latent * lax.rsqrt(jnp.mean(latent * latent, axis=1, keepdims=True) + EPS) * lgain
    kv = dot(latent.astype(BF16), lup[...])
    k_nope = kv[:, 0:128].astype(BF16)
    v_t = jnp.transpose(kv[:, 128:256]).astype(BF16)
    for h in range(2):
        r, p0 = 256 * h, 128 * h
        kvbuf[z, r : r + 128, :] = k_nope[p0 : p0 + 128]
        kvbuf[z, r + 128 : r + 256, :] = v_t[:, p0 : p0 + 128]

    for k in range(HALF):
        pl.when(sends_up)(lambda: forward(0, z, 0, k))
        pl.when(z <= DOWN)(lambda: forward(0, z, 1, PIECES - 1 - k))

    row = lax.broadcasted_iota(jnp.int32, (TOK, 128), 0)
    pl.when(z > 0)(lambda: arrived(halo_rx, h_sem.at[1]))
    behind = jnp.where(z > 0, halo_rx[...].astype(F32), 0.0)
    recur = recur.astype(F32)
    conv_sum = None
    for tap in range(4):
        back = 3 - tap
        if back:
            moved = pltpu.roll(recur, back, 0)
            edge = pltpu.roll(behind, back, 0)
            edge = jnp.concatenate([edge[0:8], moved[8:TOK]], axis=0)
            term = jnp.where(row < back, edge, moved)
        else:
            term = recur
        term = conv[tap : tap + 1, :] * term
        conv_sum = term if conv_sum is None else conv_sum + term
    conv_out = conv_sum.astype(BF16)
    zb = jnp.zeros((64, 64), BF16)

    def diagonal(w):
        return jnp.concatenate(
            [jnp.concatenate([w[0], zb], axis=1), jnp.concatenate([zb, w[1]], axis=1)], axis=0
        )

    recur_rate = jax.nn.sigmoid(dot(conv_out, diagonal(blocks[0:2])))
    input_rate = jax.nn.sigmoid(dot(conv_out, diagonal(blocks[2:4])))
    shift = jnp.concatenate(
        [
            jnp.transpose(jnp.broadcast_to(small[k : k + 1, :], (128, 128)))
            for k in (2, 3)
        ],
        axis=0,
    )
    log_decay = -8.0 * recur_rate * small[0:1, :] + shift
    a = jnp.exp(log_decay)
    b = jnp.sqrt(minus_expm1(2.0 * log_decay)) * input_rate * conv_out.astype(F32)
    for back in (1, 2, 4, 8, 16, 32, 64, 128):
        inside = row >= back
        a_before = jnp.where(inside, pltpu.roll(a, back, 0), 1.0)
        b_before = jnp.where(inside, pltpu.roll(b, back, 0), 0.0)
        b = a * b_before + b
        a = a * a_before
    a_s[...] = a
    b_s[...] = b
    rope_step(1)
    for k in range(HALF):
        pl.when(sends_up)(lambda: forward(0, z, 0, HALF + k))
        pl.when(z < DOWN)(lambda: forward(0, z, 1, HALF - 1 - k))
    cbuf[z] = jnp.concatenate([a[TOK - 1 : TOK], b[TOK - 1 : TOK]], axis=0)
    pl.when(sends_up)(lambda: carry_on(0, z, 0))
    pl.when(z < DOWN)(lambda: carry_on(0, z, 1))

    to_exp2 = float(192 ** -0.5 * np.log2(np.e))

    def scores(slot, h):
        r = 256 * h
        rope = ropebuf[slot, 64 * h : 64 * h + 64, :]
        s = dot(kvbuf[slot, r : r + 128, :], qn_s[...])
        s = s + jnp.concatenate([dot(rope, qlo_s[...]), dot(rope, qhi_s[...])], axis=0)
        return s * to_exp2

    def values(slot, h, weights):
        r = 256 * h
        return dot(kvbuf[slot, r + 128 : r + 256, :], weights.astype(BF16))

    key = lax.broadcasted_iota(jnp.int32, (128, TOK), 0)
    query = lax.broadcasted_iota(jnp.int32, (128, TOK), 1)
    s = [jnp.where(key + 128 * h <= query, scores(z, h), -jnp.inf) for h in range(2)]
    m = jnp.maximum(jnp.max(s[0], axis=0, keepdims=True), jnp.max(s[1], axis=0, keepdims=True))
    w = [jnp.exp2(v - m) for v in s]
    ml_s[0:1, :] = m
    ml_s[1:2, :] = jnp.sum(w[0] + w[1], axis=0, keepdims=True)
    acc_s[...] = values(z, 0, w[0]) + values(z, 1, w[1])

    def attend(step, slot, direction):
        @pl.when(slot < z)
        def _():
            arrived(ropebuf.at[slot, 0:112, :], s_rsem.at[direction, step])
            s = [scores(slot, h) for h in range(2)]
            old = ml_s[0:1, :]
            m = jnp.maximum(old, jnp.max(jnp.maximum(s[0], s[1]), axis=0, keepdims=True))
            w = [jnp.exp2(v - m) for v in s]
            rescale = jnp.exp2(old - m)
            ml_s[0:1, :] = m
            ml_s[1:2, :] = ml_s[1:2, :] * rescale + jnp.sum(w[0] + w[1], axis=0, keepdims=True)
            acc_s[...] = acc_s[...] * rescale + (values(slot, 0, w[0]) + values(slot, 1, w[1]))

    def step(s, before, last=False):
        up, dn = zat(-s), zat(s)
        has_up, has_dn = s <= z, dn < DOWN
        for k in range(PIECES):
            q = PIECES - 1 - k

            if k < HALF or not last:

                @pl.when(has_up)
                def _():
                    arrived(piece_at(up, k), upkv_rsem.at[s - 1, k])
                    if not last:
                        goes = sends_up & (s < DOWN) if k >= HALF else sends_up
                        pl.when(goes)(lambda: forward(s, up, 0, k))

                @pl.when((dn <= DOWN) if k < HALF else has_dn)
                def _():
                    arrived(piece_at(dn, q), dnkv_rsem.at[s - 1, q])
                    if not last:
                        if k < HALF:
                            forward(s, dn, 1, q)
                        else:
                            pl.when(s < DOWN)(lambda: forward(s, dn, 1, q))

            if before and k == 1:
                attend(s - 2, zat(1 - s), 0)
            if before and k == 3:
                attend(s - 2, zat(s - 1), 1)
            if k == 2 and not last:
                rope_step(s + 1)

        @pl.when(has_up)
        def _():
            arrived(cbuf.at[up], c_rsem.at[0, s - 1])
            if not last:
                pl.when(sends_up)(lambda: carry_on(s, up, 0))

        if not last:

            @pl.when(has_dn)
            def _():
                arrived(cbuf.at[dn], c_rsem.at[1, s - 1])
                pl.when(s < DOWN)(lambda: carry_on(s, dn, 1))

    offsets = (2, 1, -1, 0)

    def finish():
        def folded(j, state):
            return cbuf[j, 0:1, :] * state + cbuf[j, 1:2, :]

        incoming = lax.fori_loop(0, z, folded, small[1:2, :])
        xrow[:, 0:128] = ((b_s[...] + a_s[...] * incoming) * gate_s[...]).astype(BF16)
        attended = jnp.transpose(acc_s[...] / ml_s[1:2, :])
        xrow[:, 128:256] = (attended * agate_s[...]).astype(BF16)
        for side, cc in enumerate((1 - c, c)):
            for k, o in enumerate(offsets):
                at = pl.multiple_of(32 * tp_of(chip(o), cc), 32)
                xcat[side, 32 * k : 32 * k + 32, :] = xrow[pl.ds(at, 32), :]
        d2d_tx[...] = dot(xcat[0], wo[...]).astype(BF16)
        for k in range(4):
            part = slice(32 * k, 32 * k + 32)
            send(d2d_tx.at[part, :], d2d_rx.at[part, :], o_ssem, o_rsem.at[k], partner)
        psum[...] = dot(xcat[1], wo[...])

    def ship(k, value, to):
        width = value.shape[1]
        rtx[k, :, 0:width] = value.astype(BF16)
        send(rtx.at[k, :, 0:width], rrx.at[k, :, 0:width], r_ssem, r_rsem.at[k], to)

    def landed(k, width=512):
        arrived(rrx.at[k, :, 0:width], r_rsem.at[k])
        return rrx[k, :, 0:width].astype(F32)

    def add_partner(k):
        part = slice(32 * k, 32 * k + 32)
        arrived(d2d_rx.at[part, :], o_rsem.at[k])
        both = psum[part, :] + d2d_rx[part, :].astype(F32)
        psum[part, :] = both
        return both

    def reduce_first():
        two = add_partner(0)
        ship(0, two[:, 0:512], xup)
        ship(5, two[:, 1024:1536], xdn)
        ship(1, two[:, 512:1024], xup)
        ship(6, two[:, 1536:2048], xdn)
        ship(2, add_partner(1)[:, 1024:2048], xup)
        ship(7, add_partner(2)[:, 0:1024], xdn)

    def reduce_second():
        for k in range(2):
            at = 512 * k
            ship(3 + k, psum[32:64, at : at + 512] + landed(k), xup)
            ship(8 + k, psum[64:96, 1024 + at : 1536 + at] + landed(5 + k), xdn)

    def reduce_last():
        add_partner(3)
        direct = (landed(7, 1024), landed(2, 1024))
        for k in range(2):
            for side in range(2):
                at = 1024 * side + 512 * k
                total = psum[96:128, at : at + 512] + direct[side][:, 512 * k : 512 * k + 512]
                out_ref[:, at : at + 512] = (total + landed((3, 8)[side] + k)).astype(BF16)

    def between(when, stage):
        pl.when((z == 0) & when)(stage)

    pl.when(z == 0)(finish)
    step(1, False)
    pl.when(z == 0)(reduce_first)

    def middle(s, _):
        step(s, True)
        between(s == 3, reduce_second)
        between(s == 5, reduce_last)
        return 0

    lax.fori_loop(2, UP, middle, 0)
    step(UP, True, last=True)
    attend(UP - 1, zat(-UP), 0)

    @pl.when(z > 0)
    def _():
        finish()
        reduce_first()
        reduce_second()
        reduce_last()


    @pl.when(sends_up)
    def _():
        sent(halo_tx, h_sem.at[0])

    def drain(s, _):
        dn = zat(s)
        half, block = pl.ds(0, 256), pl.ds(0, 528)

        @pl.when(sends_up & (s <= z))
        def _():
            pl.when(s < DOWN)(lambda: sent(kvbuf.at[0, block, :], up_ssem.at[s]))
            pl.when(s == DOWN)(lambda: sent(kvbuf.at[0, pl.ds(0, 272), :], up_ssem.at[s]))
            sent(cbuf.at[0], c_ssem.at[0, s])

        whole = (dn < DOWN) & (s < DOWN)

        @pl.when(whole)
        def _():
            sent(kvbuf.at[0, block, :], dn_ssem.at[s])
            sent(cbuf.at[0], c_ssem.at[1, s])

        pl.when((dn <= DOWN) & jnp.logical_not(whole))(
            lambda: sent(kvbuf.at[0, half, :], dn_ssem.at[s])
        )
        pl.when(zat(-1 - s) < z)(lambda: sent(ropebuf.at[0, 0:112, :], s_ssem.at[0, s]))
        pl.when((zat(1 + s) < z) & (s < DOWN))(
            lambda: sent(ropebuf.at[0, 0:112, :], s_ssem.at[1, s])
        )
        return 0

    lax.fori_loop(0, UP, drain, 0)
    sent(xbuf.at[0:224, :], x_ssem)
    sent(latbuf.at[0:7, :, :], l_ssem)
    sent(d2d_tx, o_ssem)
    sent(rtx.at[0:6, :, :], r_ssem)


def body(
    tokens, norm_gain, recurrent_input, recurrent_gate, attention_gate, query_proj, latent_down,
    rope_key_down, conv_kernel, recurrence_gate_blocks, input_gate_blocks, decay_rate,
    decay_shift, initial_state, latent_gain, latent_up, query_gain, recurrent_output,
    attention_output,
):
    base, far = (jnp.asarray(v) for v in rotary_tables())

    def row(v):
        return v.reshape(1, -1)

    operands = (
        tokens, row(norm_gain), recurrent_input, recurrent_gate, attention_gate, query_proj.T,
        latent_down.T, rope_key_down.T, conv_kernel, recurrence_gate_blocks, input_gate_blocks,
        row(decay_rate), decay_shift.reshape(2, 128), row(initial_state),
        latent_gain.reshape(4, 128), latent_up,
        row(query_gain), recurrent_output, attention_output, base, far,
    )
    dma, vmem = pltpu.SemaphoreType.DMA, pltpu.VMEM
    scratch = [
        vmem((32, D), BF16), vmem((1, D), F32), vmem((D, 512), BF16), vmem((D, 256), BF16),
        vmem((384, D), BF16), vmem((4, 128), F32), vmem((4, 64, 64), BF16), vmem((8, 128), F32),
        vmem((512, 256), BF16), vmem((1, 192), F32), vmem((256, D), BF16),
        vmem((TOK + NZ, 256), F32),
        vmem((TOK, D), BF16), vmem((TOK, 128), BF16), vmem((8, 128, 128), BF16),
        vmem((16, 128), BF16), vmem((16, 128), BF16), vmem((NZ, 528, 128), BF16),
        vmem((NZ, 2, 128), F32), vmem((128, TOK), BF16), vmem((128, TOK), BF16),
        vmem((128, TOK), BF16), vmem((128, TOK), F32), vmem((8, TOK), F32),
        vmem((TOK, 128), F32), vmem((TOK, 128), F32), vmem((TOK, 128), F32),
        vmem((TOK, 128), F32), vmem((TOK, 256), BF16), vmem((2, 128, 256), BF16),
        vmem((128, D), BF16), vmem((128, D), BF16), vmem((128, D), F32),
        vmem((10, 32, 1024), BF16), vmem((10, 32, 1024), BF16), vmem((NZ, 128, 128), BF16),
        dma((11,)), dma(()), dma((5,)), dma((5,)), dma((2,)), dma(()), dma((4,)), dma(()),
        dma((2,)), dma((8,)), dma((8,)), dma((8, PIECES)), dma((8, PIECES)), dma((2, 8)),
        dma((2, 8)), dma((2, 8)), dma((2, 8)), dma((2, 8)), dma(()), dma((4,)), dma(()), dma((10,)),
    ]
    return pl.pallas_call(
        kernel,
        out_shape=pltpu.VMEM((32, D), BF16),
        in_specs=[pl.BlockSpec(memory_space=pl.ANY)] * len(operands),
        scratch_shapes=scratch,
        compiler_params=pltpu.CompilerParams(
            collective_id=0, has_side_effects=True, vmem_limit_bytes=56 * 2**20
        ),
    )(*operands)


def solution(mesh):
    return jax.shard_map(
        body,
        mesh=mesh,
        in_specs=(
            P(("fs", "sp", "tp"), None), P(), P(None, "tp"), P(None, "tp"), P(None, "tp"),
            P(None, "tp"), P(None, "tp"), P(), P(None, "tp"), P("tp", None, None),
            P("tp", None, None), P("tp"), P(("fs", "sp")), P(("fs", "tp")), P(), P(None, "tp"),
            P(), P("tp", None), P("tp", None),
        ),
        out_specs=P(("fs", "sp", "tp"), None),
        check_vma=False,
    )
```
